32 devices in a mesh: sp: 4 (over z), fs: 4 (over y, x), tp: 2 (over core).
Axes of the slice: x: 2, y: 2, z: 4, core: 2. Of those that a mesh axis runs over, the one named last changes fastest.
Arguments:
- tokens: bfloat16 [4, 1024, 2048], P('fs', 'sp', 'tp'), may hold values from -6 to 6
- norm_gain: float32 [2048], replicated, may hold values from 0.1 to 1.9
- memory_query: bfloat16 [2048, 1024], P('fs', 'tp'), may hold values from -0.125 to 0.125
- memory_key: bfloat16 [2048, 1024], P('fs', 'tp'), may hold values from -0.125 to 0.125
- memory_value: bfloat16 [2048, 1024], P('fs', 'tp'), may hold values from -0.125 to 0.125
- memory_outgate: bfloat16 [2048, 1024], P('fs', 'tp'), may hold values from -0.125 to 0.125
- memory_ingate: bfloat16 [2048, 4], P(None, 'tp'), may hold values from -0.125 to 0.125
- memory_forget: bfloat16 [2048, 4], P(None, 'tp'), may hold values from -0.125 to 0.125
- forget_bias: float32 [4], P('tp'), may hold values from 3 to 13
- forget_shift: float32 [4, 1024, 4], P('fs', 'sp', 'tp'), may hold values from -1.6 to 0
- stick_query: bfloat16 [2048, 512], P(None, 'tp'), may hold values from -0.125 to 0.125
- stick_key: bfloat16 [2048, 512], P(None, 'tp'), may hold values from -0.125 to 0.125
- stick_value: bfloat16 [2048, 512], P(None, 'tp'), may hold values from -0.125 to 0.125
- stick_bias: float32 [4], P('tp'), may hold values from -11 to -2
- memory_gain: float32 [1024], P('tp'), may hold values from 0.1 to 1.9
- stick_gain: float32 [512], P('tp'), may hold values from 0.1 to 1.9
- out_memory: bfloat16 [1024, 2048], P('tp'), may hold values from -0.15625 to 0.15625
- out_stick: bfloat16 [512, 2048], P('tp'), may hold values from -0.15625 to 0.15625
Outputs:
- mixed: bfloat16 [4, 1024, 2048], P('fs', ('sp', 'tp'))
The draws below stay inside these ranges and needn't reach their ends.
All inputs are finite; a program needn't handle non-finite values.
Results may differ from the reference program's by a relative error of at most 0.015.
Values may be sent and summed in bfloat16 or wider, within the bound.
A program may use at most 128 MiB of HBM per device.

```python
import jax
import jax.numpy as jnp
from jax import lax

D = 2048
HM = 4
DM = 256
HS = 4
DS = 128
TOK_DEV = 256
BLOCK = 128
SEQ = 1024
SEQS = 4
N_SP = 4


def draw_forget_bias(key, part):
    keys = jax.random.split(jax.random.fold_in(key, 11), 3)
    order = jax.random.permutation(keys[0], HM)
    fast_value = jax.random.uniform(keys[1], (HM,), jnp.float32, 3.0, 4.5)
    slow_value = jnp.log(jnp.float32(SEQ)) + jax.random.uniform(keys[2], (HM,), jnp.float32, 1.0, 2.0)
    return jnp.where(order < HM // 2, slow_value, fast_value)


def draw_forget_shift(key, part):
    keys = jax.random.split(jax.random.fold_in(key, 23), 3)
    spans = SEQ // TOK_DEV
    rate = jax.random.uniform(keys[0], (SEQS, spans, 1, HM), jnp.float32, 0.1, 1.0)
    constant_baseline = -jnp.broadcast_to(rate, (SEQS, spans, TOK_DEV, HM)).reshape(SEQS, SEQ, HM) / jnp.float32(SEQ)
    spots = jax.random.randint(keys[1], (SEQS, 3), 0, SEQ)
    layer_total = jnp.log(jax.random.uniform(keys[2], (SEQS, 3, HM), jnp.float32, 0.6, 0.8))
    pairing_tally = (jnp.arange(SEQ)[None, None, :] == spots[:, :, None]).astype(jnp.float32)
    segment_bundles = jnp.einsum('fwz,fwx->fzx', pairing_tally, layer_total)
    return constant_baseline + segment_bundles


def draw_stick_bias(key, part):
    keys = jax.random.split(jax.random.fold_in(key, 37), 3)
    order = jax.random.permutation(keys[0], HS)
    far_value = -jnp.log(jnp.float32(SEQ)) + jax.random.uniform(keys[1], (HS,), jnp.float32, -0.5, 0.5)
    near_value = jax.random.uniform(keys[2], (HS,), jnp.float32, -4.0, -2.0)
    return jnp.where(order < HS // 2, far_value, near_value)


def shard_levels(rng, dims, cuts, smallest, high):
    def one(axis_at, parts):
        draws = jax.random.uniform(jax.random.fold_in(jax.random.fold_in(rng, 6), axis_at), (parts,), jnp.float32, smallest / len(cuts), high / len(cuts))
        return jnp.repeat(jnp.exp(draws), dims[axis_at] // parts).reshape((-1,) + (1,) * (len(dims) - axis_at - 1))

    factor_of = one(*cuts[0])
    for cut in cuts[1:]:
        factor_of = factor_of * one(*cut)
    return factor_of


def centred(own_key, extent, scale, bound, pieces=(), kind=jnp.bfloat16):
    level = shard_levels(own_key, extent, pieces, -0.22, 0.18) if pieces else 1.0
    result = jax.random.normal(own_key, extent, jnp.float32) * scale * level
    return jnp.minimum(jnp.maximum(result, -bound), bound).astype(kind)


def setup_inputs(seed: int = 0) -> dict:
    key_list = jax.random.split(jax.random.key(seed), 19)
    return {
        "tokens": centred(key_list[0], (SEQS, SEQ, D), 1.0, 6.0, ((0, 4), (1, 4), (2, 2))),
        "norm_gain": jnp.clip(1.0 + 0.18 * jax.random.normal(key_list[1], (D,), jnp.float32), 0.1, 1.9),
        "memory_query": centred(key_list[2], (D, HM * DM), D ** -0.5, 0.125, ((0, 4), (1, 2))),
        "memory_key": centred(key_list[3], (D, HM * DM), D ** -0.5, 0.125, ((0, 4), (1, 2))),
        "memory_value": centred(key_list[4], (D, HM * DM), D ** -0.5, 0.125, ((0, 4), (1, 2))),
        "memory_outgate": centred(key_list[5], (D, HM * DM), D ** -0.5, 0.125, ((0, 4), (1, 2))),
        "memory_ingate": centred(key_list[6], (D, HM), D ** -0.5, 0.125, ((1, 2),)),
        "memory_forget": centred(key_list[7], (D, HM), D ** -0.5, 0.125, ((1, 2),)),
        "forget_bias": draw_forget_bias(jax.random.fold_in(key_list[18], 71), 0),
        "forget_shift": draw_forget_shift(jax.random.fold_in(key_list[18], 71), 0),
        "stick_query": centred(key_list[10], (D, HS * DS), D ** -0.5, 0.125, ((1, 2),)),
        "stick_key": centred(key_list[11], (D, HS * DS), D ** -0.5, 0.125, ((1, 2),)),
        "stick_value": centred(key_list[12], (D, HS * DS), D ** -0.5, 0.125, ((1, 2),)),
        "stick_bias": draw_stick_bias(jax.random.fold_in(key_list[18], 71), 0),
        "memory_gain": jnp.clip(1.0 + 0.18 * jax.random.normal(key_list[14], (HM * DM,), jnp.float32), 0.1, 1.9),
        "stick_gain": jnp.clip(1.0 + 0.18 * jax.random.normal(key_list[15], (HS * DS,), jnp.float32), 0.1, 1.9),
        "out_memory": centred(key_list[16], (HM * DM, D), (HM * DM + HS * DS) ** -0.5, 0.15625, ((0, 2),)),
        "out_stick": centred(key_list[17], (HS * DS, D), (HM * DM + HS * DS) ** -0.5, 0.15625, ((0, 2),)),
    }


epsilon = 1e-06
floor_neg = -1e+30
peak_value = lax.Precision.HIGHEST

def rounded(values):
    return lax.optimization_barrier(values.astype(jnp.bfloat16)).astype(jnp.float32)

def per_head_norm(values, gain):
    scale = lax.rsqrt(lax.optimization_barrier(jnp.mean(values * values, axis=-1, keepdims=True)) + epsilon)
    return values * scale * gain

def memory_block(state_carry, inputs):
    state_matrix, state_max = state_carry
    queries, key_rows, value_rows, log_forget, in_gate = inputs
    length = queries.shape[0]
    causal = jnp.tril(jnp.ones((length, length), dtype=bool))
    cumulative = jnp.cumsum(log_forget, axis=0)
    spread = cumulative[:, None, :] - cumulative[None, :, :] + in_gate[None, :, :]
    spread = jnp.where(causal[:, :, None], spread, floor_neg)
    carried_log = cumulative + state_max[None, :]
    running = jnp.maximum(carried_log, lax.optimization_barrier(jnp.max(spread, axis=1)))
    carried = jnp.exp(carried_log - running)
    scores = jnp.einsum('thd,shd->tsh', queries, key_rows, precision=peak_value) * jnp.exp(spread - running[:, None, :])
    numerator = carried[:, :, None] * jnp.einsum('thd,hde->the', queries, state_matrix, precision=peak_value)
    numerator = numerator + jnp.einsum('tsh,she->the', scores, value_rows, precision=peak_value)
    block_total = cumulative[-1]
    gap_logs = block_total[None, :] - cumulative + in_gate
    next_max = jnp.maximum(block_total + state_max, lax.optimization_barrier(jnp.max(gap_logs, axis=0)))
    decay_factor = jnp.exp(block_total + state_max - next_max)
    weights = jnp.exp(gap_logs - next_max[None, :])
    next_matrix = decay_factor[:, None, None] * state_matrix + jnp.einsum('sh,shd,she->hde', weights, key_rows, value_rows, precision=peak_value)
    return ((next_matrix, next_max), numerator)

def memory_mixer(queries, key_rows, value_rows, log_forget, in_gate):
    segment_list = SEQ // BLOCK

    def split_blocks(array):
        return array.reshape((segment_list, BLOCK) + array.shape[1:])
    initial = (jnp.zeros((HM, DM, DM), jnp.float32), jnp.full((HM,), floor_neg, jnp.float32))
    scaled = key_rows * DM ** (-0.5)
    _, outputs = lax.scan(memory_block, initial, (split_blocks(queries), split_blocks(scaled), split_blocks(value_rows), split_blocks(log_forget), split_blocks(in_gate)))
    return outputs.reshape(SEQ, HM, DM)

def stick_piece(queries, key_rows, value_rows, head_bias, query_pos, key_start):
    logits = jnp.einsum('thd,shd->hts', queries.astype(jnp.float32), key_rows.astype(jnp.float32), precision=peak_value)
    logits = logits * DS ** (-0.5) + head_bias[:, None, None]
    key_pos = key_start + jnp.arange(key_rows.shape[0], dtype=jnp.int32)
    visible = key_pos[None, :] < query_pos[:, None]
    keep_log = jnp.where(visible[None], jax.nn.log_sigmoid(-logits), jnp.float32(0.0))
    after = lax.cumsum(keep_log, axis=2, reverse=True) - keep_log
    weights = jnp.where(visible[None], jnp.exp(jax.nn.log_sigmoid(logits) + after), jnp.float32(0.0)).astype(jnp.bfloat16)
    partial_out = jnp.einsum('hts,shd->thd', weights.astype(jnp.float32), value_rows.astype(jnp.float32), precision=peak_value)
    return (partial_out, lax.optimization_barrier(jnp.sum(keep_log, axis=2)).T)

def stick_mixer(queries, key_rows, value_rows, head_bias):

    def span_out(span):
        first_row = span * TOK_DEV
        query_span = lax.dynamic_slice_in_dim(queries, first_row, TOK_DEV, 0)
        query_pos = first_row + jnp.arange(TOK_DEV, dtype=jnp.int32)

        def visit(offset, state_carry):
            accumulated, running_sum = state_carry
            key_start = ((span - offset) * TOK_DEV).astype(jnp.int32)
            keys_span = lax.dynamic_slice_in_dim(key_rows, key_start, TOK_DEV, 0)
            values_span = lax.dynamic_slice_in_dim(value_rows, key_start, TOK_DEV, 0)
            part_out, part_keep = stick_piece(query_span, keys_span, values_span, head_bias, query_pos, key_start)
            return (accumulated + jnp.exp(running_sum)[:, :, None] * part_out, running_sum + part_keep)
        initial = (jnp.zeros((TOK_DEV, HS, DS), jnp.float32), jnp.zeros((TOK_DEV, HS), jnp.float32))
        accumulated, _ = lax.fori_loop(0, span + 1, visit, initial)
        return accumulated
    outputs = lax.map(span_out, jnp.arange(N_SP, dtype=jnp.int32))
    return outputs.reshape(SEQ, HS, DS)

def reference(tokens, norm_gain, memory_query, memory_key, memory_value, memory_outgate, memory_ingate, memory_forget, forget_bias, forget_shift, stick_query, stick_key, stick_value, stick_bias, memory_gain, stick_gain, out_memory, out_stick):

    def one_sequence(inputs):
        rows_in, shift_rows = inputs
        values = rows_in.astype(jnp.float32)
        normed = (values * lax.rsqrt(lax.optimization_barrier(jnp.mean(values * values, axis=-1, keepdims=True)) + epsilon) * norm_gain).astype(jnp.bfloat16)

        def project(weight):
            return jnp.dot(normed, weight, preferred_element_type=jnp.float32)
        memory_shape = (SEQ, HM, DM)
        queries = rounded(project(memory_query)).reshape(memory_shape)
        key_rows = rounded(project(memory_key)).reshape(memory_shape)
        value_rows = rounded(project(memory_value)).reshape(memory_shape)
        out_gate = jax.nn.sigmoid(rounded(project(memory_outgate))).reshape(memory_shape)
        in_gate = project(memory_ingate)
        log_forget = jax.nn.log_sigmoid(project(memory_forget) + forget_bias) + shift_rows
        memory_out = memory_mixer(queries, key_rows, value_rows, log_forget, in_gate)
        mix_memory = per_head_norm(out_gate * memory_out, memory_gain.reshape(HM, DM)).reshape(SEQ, HM * DM).astype(jnp.bfloat16)
        stick_shape = (SEQ, HS, DS)
        stick_q = project(stick_query).astype(jnp.bfloat16).reshape(stick_shape)
        stick_k = project(stick_key).astype(jnp.bfloat16).reshape(stick_shape)
        stick_v = project(stick_value).astype(jnp.bfloat16).reshape(stick_shape)
        stick_out = stick_mixer(stick_q, stick_k, stick_v, stick_bias)
        mix_stick = per_head_norm(stick_out, stick_gain.reshape(HS, DS)).reshape(SEQ, HS * DS).astype(jnp.bfloat16)
        mixed = jnp.dot(mix_memory, out_memory, preferred_element_type=jnp.float32) + jnp.dot(mix_stick, out_stick, preferred_element_type=jnp.float32)
        return mixed.astype(jnp.bfloat16)
    return lax.map(one_sequence, (tokens, forget_shift))
```

```python
import functools

import jax
import jax.numpy as jnp
from jax import lax
from jax.experimental import pallas as pl
from jax.experimental.pallas import tpu as pltpu
from jax.sharding import PartitionSpec as P

MESH = pl.DeviceIdType.MESH
epsilon = 1e-06
floor_neg = -1e30
f32 = jnp.float32
bf16 = jnp.bfloat16

KEY, VALUE, QUERY, GATE = 0, 1, 2, 3


def dot(a, b, dims=((1,), (0,))):
    return lax.dot_general(a, b, (dims, ((), ())), preferred_element_type=f32)


def softplus(z):
    return jnp.maximum(z, 0.0) + jnp.log(1.0 + jnp.exp(-jnp.abs(z)))


def kernel(
    n_sp,
    n_out,
    tok_hbm,
    gain_hbm,
    ingate_hbm,
    forget_hbm,
    bias_ref,
    shift_hbm,
    sbias_ref,
    mgain_hbm,
    sgain_hbm,
    wk_hbm,
    wv_hbm,
    wq_hbm,
    wo_hbm,
    sq_hbm,
    sk_hbm,
    sv_hbm,
    om_hbm,
    os_hbm,
    out_ref,
    tok_ref,
    gain_ref,
    ingate_ref,
    forget_ref,
    shift_ref,
    mgain_ref,
    sgain_ref,
    tok_in,
    nrm,
    xg,
    wm,
    wg,
    ws,
    wout,
    sb,
    rb,
    own_part,
    proj,
    queries,
    kv,
    stick_acc,
    stick_run,
    far_out,
    far_in,
    gw,
    u_rows,
    u_cols,
    totals,
    tops,
    state_own,
    state_in,
    state_out,
    log_in,
    log_out,
    mix,
    early_out,
    ob,
    orb,
    load_sem,
    tok_s,
    tok_r,
    a2a_s,
    a2a_r,
    fwd_s,
    fwd_r,
    w_s,
    w_r,
    pass_s,
    z_r,
    rs_s,
    rs_r,
    kv_s,
    kv_r,
    far_s,
    far_r,
    chain_s,
    chain_r,
    log_s,
    log_r,
    out_s,
    out_r,
):
    f = lax.axis_index("fs")
    s = lax.axis_index("sp")
    t = lax.axis_index("tp")
    rows, half_feat = tok_ref.shape
    heads = state_own.shape[0]
    dm = state_own.shape[1]
    ds = sgain_ref.shape[1] // heads
    block = wm.shape[1]
    half = rows // 2
    other = 1 - t
    last = n_sp - 1
    helper = n_sp - 2

    def flip(bits):
        if bits == 1:
            return f + 1 - 2 * (f % 2)
        if bits == 2:
            return f + 2 - 4 * (f // 2)
        return 3 - f

    def remote(src, dst, send, recv, device):
        return pltpu.make_async_remote_copy(
            src_ref=src,
            dst_ref=dst,
            send_sem=send,
            recv_sem=recv,
            device_id=device,
            device_id_type=MESH,
        )

    barrier = pltpu.get_barrier_semaphore()
    pl.semaphore_signal(barrier, inc=1, device_id={"tp": other}, device_id_type=MESH)
    for bits in (1, 2):
        pl.semaphore_signal(barrier, inc=1, device_id={"fs": flip(bits)}, device_id_type=MESH)

    @pl.when(s > 0)
    def _():
        pl.semaphore_signal(barrier, inc=1, device_id={"sp": s - 1}, device_id_type=MESH)

    @pl.when(s < last)
    def _():
        pl.semaphore_signal(barrier, inc=1, device_id={"sp": s + 1}, device_id_type=MESH)

    def load(src, dst, at):
        return pltpu.make_async_copy(src, dst, load_sem.at[at])

    load(tok_hbm, tok_ref, 0).start()
    load(wk_hbm, wm.at[KEY], 1).start()
    load(wv_hbm, wm.at[VALUE], 1).start()
    load(gain_hbm, gain_ref, 2).start()
    load(sq_hbm, ws.at[0], 3).start()
    load(wq_hbm, wm.at[QUERY], 4).start()
    load(wo_hbm, wm.at[GATE], 4).start()
    load(sk_hbm, ws.at[1], 5).start()
    load(sv_hbm, ws.at[2], 5).start()
    load(ingate_hbm, ingate_ref, 6).start()
    load(forget_hbm, forget_ref, 7).start()
    load(shift_hbm, shift_ref, 8).start()
    load(om_hbm, wout.at[pl.ds(0, heads * dm)], 9).start()
    load(os_hbm, wout.at[pl.ds(heads * dm, heads * ds)], 9).start()
    load(mgain_hbm, mgain_ref, 10).start()
    load(sgain_hbm, sgain_ref, 11).start()

    def loaded(ref, at):
        pltpu.make_async_copy(ref, ref, load_sem.at[at]).wait()

    peers = 3 + jnp.where(s > 0, 1, 0) + jnp.where(s < last, 1, 0)
    pl.semaphore_wait(barrier, peers)

    loaded(tok_ref, 0)
    tok_copy = remote(tok_ref, tok_in, tok_s.at[0], tok_r.at[0], {"tp": other})
    tok_copy.start()

    def role(p, h):
        return (p + h) % 2

    def pair_bits(p, h):
        return 1 + role(p, h)

    def sum_bits(p, h):
        return 2 - role(p, h)

    first, second = [(KEY, 0), (VALUE, 0)], [(KEY, 1), (VALUE, 1)]
    third, fourth = [(QUERY, h) for h in range(heads)], [(GATE, h) for h in range(heads)]
    lines_p = block // 2
    parity = pl.ds(pl.multiple_of((s % 2) * lines_p, lines_p), lines_p)
    rest = pl.ds(pl.multiple_of((1 - s % 2) * lines_p, lines_p), lines_p)

    def stage(p, h):
        return h if p < 2 else p

    def weight_copy(p, h):
        return remote(
            wm.at[p, parity, pl.ds(h * dm, dm)], wg.at[p, h, parity], w_s.at[0],
            w_r.at[stage(p, h)], {"fs": flip(pair_bits(p, h))},
        )

    def rest_copy(p, h):
        return remote(
            wm.at[p, rest, pl.ds(h * dm, dm)], wg.at[p, h, rest], w_s.at[1],
            w_r.at[4], {"fs": flip(pair_bits(p, h))},
        )

    def pass_copy(p, h, at, to):
        return remote(
            wg.at[p, h, parity], wg.at[p, h, parity], pass_s.at[at], z_r.at[stage(p, h)], {"sp": to}
        )

    def both(p, h, lines):
        return wg.at[pl.ds(0, 2), h, lines] if p < 2 else wg.at[p, :, lines]

    def await_bytes(ref, sem):
        remote(ref, ref, pass_s.at[0], sem, {"tp": other}).wait_recv()

    def sent_bytes(ref, sem):
        remote(ref, ref, sem, z_r.at[0], {"tp": other}).wait_send()

    def send_weights(items):
        for p, h in items:
            weight_copy(p, h).start()

    def pass_weights(items):
        p, h = items[0]
        await_bytes(both(p, h, parity), w_r.at[stage(p, h)])
        for p, h in items:
            @pl.when(s > 0)
            def _():
                pass_copy(p, h, 0, s - 1).start()

            if p != GATE:
                @pl.when(s == helper)
                def _():
                    pass_copy(p, h, 1, s + 1).start()

    def rest_weights(items):
        p, h = items[0]
        if p != GATE:
            await_bytes(both(p, h, rest), z_r.at[stage(p, h)])
            return

        @pl.when(s < last)
        def _():
            await_bytes(both(p, h, rest), z_r.at[stage(p, h)])

        @pl.when(s == last)
        def _():
            await_bytes(both(p, h, rest), w_r.at[4])

    loaded(wm.at[pl.ds(KEY, 2)], 1)
    send_weights(first)
    send_weights(second)
    tok_copy.wait_recv()
    loaded(gain_ref, 2)

    step_rows = 32
    own_cols = pl.ds(pl.multiple_of(t * half_feat, half_feat), half_feat)
    far_cols = pl.ds(pl.multiple_of(other * half_feat, half_feat), half_feat)

    def norm_rows(i, _):
        at = pl.ds(pl.multiple_of(i * step_rows, step_rows), step_rows)
        own = tok_ref[at, :].astype(f32)
        far = tok_in[at, :].astype(f32)
        total = jnp.sum(own * own, axis=1, keepdims=True) + jnp.sum(far * far, axis=1, keepdims=True)
        scale = lax.rsqrt(total / (2 * half_feat) + epsilon)
        nrm[at, own_cols] = (own * scale * gain_ref[:, own_cols]).astype(bf16)
        nrm[at, far_cols] = (far * scale * gain_ref[:, far_cols]).astype(bf16)
        return 0

    lax.fori_loop(0, rows // step_rows, norm_rows, 0)

    my_rows = pl.ds(pl.multiple_of(t * half, half), half)

    def feature_block(index):
        return pl.ds(pl.multiple_of(index * block, block), block)

    a2a, fwd = {}, {}
    for r in range(2):
        for which in range(2):
            at = r * 2 + which
            to = flip(2 - r)
            a2a[at] = remote(
                nrm.at[my_rows, feature_block(to if which == 0 else flip(3))],
                xg.at[r, which, my_rows],
                a2a_s.at[0],
                a2a_r.at[at],
                {"fs": to},
            )
            a2a[at].start()
    loaded(wm.at[pl.ds(QUERY, 2)], 4)
    send_weights(third)
    send_weights(fourth)

    loaded(ws.at[0], 3)
    normed = nrm[...]
    queries[0] = dot(normed, ws[0]).astype(bf16)

    def query_copy():
        return remote(queries.at[0], queries.at[1], far_s.at[0], far_r.at[0], {"sp": s - 1})

    @pl.when(s == last)
    def _():
        query_copy().start()

    pass_weights(first)
    loaded(ws.at[pl.ds(1, 2)], 5)
    kv[0, 0] = dot(normed, ws[1]).astype(bf16)
    kv[0, 1] = dot(normed, ws[2]).astype(bf16)

    def kv_copy(d):
        return remote(kv.at[d - 1], kv.at[d], kv_s.at[d], kv_r.at[d], {"sp": s + 1})

    def kv_send(d):
        @pl.when((s < helper) & (s >= d - 1))
        def _():
            kv_copy(d).start()

    kv_send(1)

    row_at = lax.broadcasted_iota(jnp.int32, (rows, rows), 0)
    col_at = lax.broadcasted_iota(jnp.int32, (rows, rows), 1)
    loaded(ingate_ref, 6)
    loaded(forget_ref, 7)
    loaded(shift_ref, 8)
    gw[...] = jnp.zeros(gw.shape, bf16)
    gw[0:heads, :] = ingate_ref[...]
    gw[8 : 8 + heads, :] = forget_ref[...]
    gate = dot(gw[...], normed, ((1,), (1,)))
    triu = (row_at <= col_at).astype(f32)
    u_rows[...] = jnp.zeros(u_rows.shape, f32)
    for h in range(heads):
        log_forget = shift_ref[h : h + 1, :] - softplus(-(gate[8 + h : 9 + h, :] + bias_ref[h]))
        cumulative = lax.dot_general(
            jnp.broadcast_to(log_forget, (8, rows)), triu, (((1,), (0,)), ((), ())),
            precision=lax.Precision.HIGHEST, preferred_element_type=f32,
        )
        u_rows[h : h + 1, :] = gate[h : h + 1, :] - cumulative[0:1, :]
        totals[h : h + 1, :] = jnp.broadcast_to(
            cumulative[0:1, rows - 1 : rows], (1, totals.shape[1])
        )
    u_cols[...] = jnp.transpose(u_rows[...])
    pass_weights(second)

    def stick_part(at, h, kv_at, diagonal):
        cols = slice(h * ds, (h + 1) * ds)
        z = dot(queries[at, :, cols], kv[kv_at, 0, :, cols], ((1,), (1,)))
        z = z * ds ** (-0.5) + sbias_ref[h]
        keep = -softplus(z)
        visible = col_at < row_at
        if diagonal:
            kept = jnp.where(visible, keep, 0.0)
        else:
            kept = keep
        strict = (row_at > col_at).astype(bf16)
        high = kept.astype(bf16)
        low = (kept - high.astype(f32)).astype(bf16)
        after = dot(high, strict) + dot(low, strict)
        weights = jnp.exp(z + keep + after)
        if diagonal:
            weights = jnp.where(visible, weights, 0.0)
        part = dot(weights.astype(bf16), kv[kv_at, 1, :, cols])
        return part, jnp.sum(kept, axis=1, keepdims=True)

    def stick_first(at, diagonal):
        for h in range(heads):
            part, keep = stick_part(at, h, 0, diagonal)
            stick_acc[at, h] = part
            stick_run[at, h] = jnp.broadcast_to(keep, stick_run.shape[2:])

    def kv_forward(d):
        @pl.when((s >= d) & (s <= helper))
        def _():
            remote(kv.at[d - 1], kv.at[d], kv_s.at[d], kv_r.at[d], {"sp": s - 1}).wait_recv()

        @pl.when((s >= d) & (s < helper))
        def _():
            kv_copy(d + 1).start()

    def stick_span(d):
        @pl.when((s >= d) & (s <= helper))
        def _():
            def one(at, _):
                for h in range(heads):
                    part, keep = stick_part(at, h, d, False)
                    stick_acc[at, h] = stick_acc[at, h] + jnp.exp(stick_run[at, h]) * part
                    stick_run[at, h] = stick_run[at, h] + keep
                return 0

            lax.fori_loop(0, 1 + jnp.where(s == helper, 1, 0), one, 0)

    def over(low, high, step):
        if high > low:
            lax.fori_loop(low, high, lambda d, c: (step(d), c)[1], 0)

    stick_first(0, True)

    @pl.when(s == helper)
    def _():
        query_copy().wait_recv()
        stick_first(1, False)

    for at in (0, 2, 1, 3):
        a2a[at].wait_recv()
        r, which = divmod(at, 2)
        fwd[at] = remote(
            xg.at[r, which, my_rows],
            xg.at[r, which, my_rows],
            fwd_s.at[0],
            fwd_r.at[r],
            {"tp": other},
        )
        fwd[at].start()

    far_rows = pl.ds(pl.multiple_of(other * half, half), half)

    def rs_sem(p, h):
        return h if p < 2 else p + (h if p == GATE else 0)

    def rs_copy(p, h, lines):
        return remote(
            sb.at[p, h, lines], rb.at[p, h, lines], rs_s.at[0], rs_r.at[rs_sem(p, h)],
            {"fs": flip(sum_bits(p, h))},
        )

    def partials(items):
        rest_weights(items)
        for p, h in items:
            cols = slice(h * dm, (h + 1) * dm)
            r = role(p, h)
            sb[p, h] = (dot(xg[r, 0], wm[p, :, cols]) + dot(xg[r, 1], wg[p, h])).astype(bf16)
            rs_copy(p, h, pl.ds(0, rows)).start()

    def first_partials(items):
        rest_weights(items)
        for lines in (my_rows, far_rows):
            for p, h in items:
                cols = slice(h * dm, (h + 1) * dm)
                r = role(p, h)
                if lines is far_rows:
                    await_bytes(xg.at[r, :, far_rows], fwd_r.at[r])
                sb[p, h, lines] = (
                    dot(xg[r, 0, lines], wm[p, :, cols]) + dot(xg[r, 1, lines], wg[p, h])
                ).astype(bf16)
                rs_copy(p, h, lines).start()

    def own_partials(items):
        for p, h in items:
            cols = slice(h * dm, (h + 1) * dm)
            own_part[p, h] = dot(nrm[:, feature_block(f)], wm[p, :, cols]) + dot(
                nrm[:, feature_block(flip(pair_bits(p, h)))], wg[p, h]
            )

    def finish(p, h):
        return (own_part[p, h] + rb[p, h].astype(f32)).astype(bf16)

    def column(h):
        return u_cols[:, h : h + 1]

    def own_state(h):
        await_bytes(rb.at[pl.ds(0, 2), h], rs_r.at[h])
        proj[KEY, h] = (finish(KEY, h).astype(f32) * dm ** (-0.5)).astype(bf16)
        proj[VALUE, h] = finish(VALUE, h)
        u = column(h)
        top = jnp.max(u, axis=0, keepdims=True)
        weighted = (proj[KEY, h].astype(f32) * jnp.exp(u - top)).astype(bf16)
        state_own[h] = dot(weighted, proj[VALUE, h], ((0,), (0,)))

    def log_copy(h, to):
        return remote(log_out.at[h], log_in.at[h], log_s.at[0], log_r.at[h], {"sp": to})

    piece_dm = dm // 2
    pieces = 4

    def chain_copy(h, c, to):
        lines = pl.ds(c // 2 * piece_dm, piece_dm)
        cols = pl.ds(c % 2 * piece_dm, piece_dm)
        at = h * pieces + c
        return remote(
            state_out.at[h, lines, cols], state_in.at[h, lines, cols], chain_s.at[0], chain_r.at[at],
            {"sp": to},
        )

    def chain(h):
        @pl.when(s == 0)
        def _():
            log_in[h] = jnp.full(log_in.shape[1:], floor_neg, f32)
            state_in[h] = jnp.zeros(state_in.shape[1:], bf16)

        @pl.when(s > 0)
        def _():
            log_copy(h, s - 1).wait_recv()

        total = totals[h : h + 1, 0:1]
        early = total + log_in[h, 0:1, 0:1]
        late = total + jnp.max(column(h), axis=0, keepdims=True)
        top = jnp.maximum(early, late)

        @pl.when(s < last)
        def _():
            log_out[h] = jnp.broadcast_to(top, log_out.shape[1:])
            log_copy(h, s + 1).start()

        early, late = jnp.exp(early - top), jnp.exp(late - top)
        for c in range(pieces):
            lines = pl.ds(c // 2 * piece_dm, piece_dm)
            cols = pl.ds(c % 2 * piece_dm, piece_dm)

            @pl.when(s > 0)
            def _():
                chain_copy(h, c, s - 1).wait_recv()

            @pl.when(s < last)
            def _():
                state_out[h, lines, cols] = (
                    early * state_in[h, lines, cols].astype(f32) + late * state_own[h, lines, cols]
                ).astype(bf16)
                chain_copy(h, c, s + 1).start()

    def chain_if(where, h):
        @pl.when(where)
        def _():
            chain(h)

    pass_weights(third)
    over(1, min(2, n_sp - 1), kv_forward)
    first_partials(first)
    own_partials(first)
    partials(second)
    own_partials(second)
    pass_weights(fourth)

    @pl.when(s == last)
    def _():
        for p, h in fourth:
            rest_copy(p, h).start()

    over(1, min(2, n_sp - 1), stick_span)
    own_state(0)
    chain_if(s == 0, 0)
    over(2, n_sp - 1, kv_forward)
    over(2, n_sp - 1, stick_span)

    @pl.when(s == helper)
    def _():
        far_out[...] = stick_acc[1].astype(bf16)
        remote(far_out, far_in, far_s.at[1], far_r.at[1], {"sp": s + 1}).start()

    own_state(1)
    chain_if(s == 0, 1)
    chain_if(s == 1, 0)
    partials(third)
    own_partials(third)
    chain_if(s == 1, 1)
    chain_if(s == 2, 0)
    partials(fourth)
    own_partials(fourth)
    loaded(wout, 9)
    loaded(mgain_ref, 10)
    loaded(sgain_ref, 11)
    chain_if(s == 2, 1)

    causal = col_at <= row_at
    await_bytes(rb.at[QUERY], rs_r.at[QUERY])
    for h in range(heads):
        proj[QUERY, h] = finish(QUERY, h)
        masked = jnp.where(causal, u_rows[h : h + 1, :], floor_neg)
        top = jnp.max(masked, axis=1, keepdims=True)
        scores = dot(proj[QUERY, h], proj[KEY, h], ((1,), (1,))) * jnp.exp(masked - top)
        own_part[QUERY, h] = dot(scores.astype(bf16), proj[VALUE, h])
        tops[h] = jnp.broadcast_to(top, tops.shape[1:])

    @pl.when(s == last)
    def _():
        remote(far_out, far_in, far_s.at[1], far_r.at[1], {"sp": s - 1}).wait_recv()
        for h in range(heads):
            stick_acc[0, h] = stick_acc[0, h] + jnp.exp(stick_run[0, h]) * far_in[h].astype(f32)

    for h in range(heads):
        cols = slice(h * ds, (h + 1) * ds)
        out = stick_acc[0, h]
        scale = lax.rsqrt(jnp.mean(out * out, axis=1, keepdims=True) + epsilon)
        mix[:, heads * dm + h * ds : heads * dm + (h + 1) * ds] = (
            out * scale * sgain_ref[:, cols]
        ).astype(bf16)
    early_out[...] = dot(mix[:, heads * dm :], wout[heads * dm :, :])

    for h in range(heads):
        chain_if(s > 2, h)
        carried_max = log_in[h, 0:1, 0:1]
        top = tops[h, :, 0:1]
        running = jnp.maximum(carried_max, top)
        own_part[QUERY, h] = jnp.exp(top - running) * own_part[QUERY, h] + jnp.exp(
            carried_max - running
        ) * dot(proj[QUERY, h], state_in[h])
        await_bytes(rb.at[GATE, h], rs_r.at[GATE + h])
        gated = own_part[QUERY, h] / (1.0 + jnp.exp(-finish(GATE, h).astype(f32)))
        scale = lax.rsqrt(jnp.mean(gated * gated, axis=1, keepdims=True) + epsilon)
        cols = slice(h * dm, (h + 1) * dm)
        mix[:, cols] = (gated * scale * mgain_ref[:, cols]).astype(bf16)
        if h < heads - 1:
            early_out[...] = early_out[...] + dot(mix[:, cols], wout[cols, :])

    piece = wout.shape[1] // n_out
    lines = slice((heads - 1) * dm, heads * dm)
    copies = []
    for c in range(n_out):
        cols = slice(c * piece, (c + 1) * piece)
        ob[c] = (early_out[far_rows, cols] + dot(mix[far_rows, lines], wout[lines, cols])).astype(bf16)
        copy = remote(ob.at[c], orb.at[c], out_s.at[0], out_r.at[c], {"tp": other})
        copy.start()
        copies.append(copy)
    for c in range(n_out):
        cols = slice(c * piece, (c + 1) * piece)
        early_out[my_rows, cols] = early_out[my_rows, cols] + dot(mix[my_rows, lines], wout[lines, cols])
    for c in range(n_out):
        cols = slice(c * piece, (c + 1) * piece)
        copies[c].wait_recv()
        out_ref[:, cols] = (early_out[my_rows, cols] + orb[c].astype(f32)).astype(bf16)

    tok_copy.wait_send()
    sent_bytes(xg.at[:, :, my_rows], a2a_s.at[0])
    sent_bytes(xg.at[:, :, my_rows], fwd_s.at[0])
    sent_bytes(wm.at[:, parity], w_s.at[0])
    sent_bytes(sb, rs_s.at[0])
    sent_bytes(ob, out_s.at[0])

    @pl.when(s > 0)
    def _():
        sent_bytes(wg.at[:, :, parity], pass_s.at[0])

    @pl.when(s == helper)
    def _():
        sent_bytes(wg.at[pl.ds(0, 3), :, parity], pass_s.at[1])
        remote(far_out, far_in, far_s.at[1], far_r.at[1], {"sp": s + 1}).wait_send()

    @pl.when(s == last)
    def _():
        query_copy().wait_send()
        sent_bytes(wm.at[GATE, rest], w_s.at[1])

    @pl.when(s < last)
    def _():
        sent_bytes(log_out, log_s.at[0])
        sent_bytes(state_out, chain_s.at[0])

    def kv_done(d, c):
        @pl.when((s < helper) & (s >= d - 1))
        def _():
            kv_copy(d).wait_send()

        return c

    lax.fori_loop(1, n_sp - 1, kv_done, 0)


def per_device(
    n_sp,
    tokens,
    norm_gain,
    memory_query,
    memory_key,
    memory_value,
    memory_outgate,
    memory_ingate,
    memory_forget,
    forget_bias,
    forget_shift,
    stick_query,
    stick_key,
    stick_value,
    stick_bias,
    memory_gain,
    stick_gain,
    out_memory,
    out_stick,
):
    rows, half_feat = tokens.shape[1:]
    features = 2 * half_feat
    heads = forget_bias.shape[0]
    block, width = memory_query.shape
    dm = width // heads
    stick_width = stick_query.shape[1]
    ds = stick_width // heads
    lanes = 128
    n_out = 4
    half = rows // 2

    vmem = pl.BlockSpec(memory_space=pltpu.VMEM)
    smem = pl.BlockSpec(memory_space=pltpu.SMEM)
    anyw = pl.BlockSpec(memory_space=pl.ANY)
    dma = pltpu.SemaphoreType.DMA
    out = pl.pallas_call(
        functools.partial(kernel, n_sp, n_out),
        out_shape=pltpu.VMEM((half, features), bf16),
        in_specs=[anyw] * 4 + [smem, anyw, smem] + [anyw] * 11,
        out_specs=vmem,
        scratch_shapes=[
            pltpu.VMEM((rows, half_feat), bf16),
            pltpu.VMEM((1, features), f32),
            pltpu.VMEM((heads, features), bf16),
            pltpu.VMEM((heads, features), bf16),
            pltpu.VMEM((heads, rows), f32),
            pltpu.VMEM((1, width), f32),
            pltpu.VMEM((1, stick_width), f32),
            pltpu.VMEM((rows, half_feat), bf16),
            pltpu.VMEM((rows, features), bf16),
            pltpu.VMEM((2, 2, rows, block), bf16),
            pltpu.VMEM((4, block, width), bf16),
            pltpu.VMEM((4, heads, block, dm), bf16),
            pltpu.VMEM((3, features, stick_width), bf16),
            pltpu.VMEM((width + stick_width, features), bf16),
            pltpu.VMEM((4, heads, rows, dm), bf16),
            pltpu.VMEM((4, heads, rows, dm), bf16),
            pltpu.VMEM((4, heads, rows, dm), f32),
            pltpu.VMEM((4, heads, rows, dm), bf16),
            pltpu.VMEM((2, rows, stick_width), bf16),
            pltpu.VMEM((n_sp - 1, 2, rows, stick_width), bf16),
            pltpu.VMEM((2, heads, rows, ds), f32),
            pltpu.VMEM((2, heads, rows, ds), f32),
            pltpu.VMEM((heads, rows, ds), bf16),
            pltpu.VMEM((heads, rows, ds), bf16),
            pltpu.VMEM((16, features), bf16),
            pltpu.VMEM((lanes, rows), f32),
            pltpu.VMEM((rows, lanes), f32),
            pltpu.VMEM((8, lanes), f32),
            pltpu.VMEM((heads, rows, lanes), f32),
            pltpu.VMEM((heads, dm, dm), f32),
            pltpu.VMEM((heads, dm, dm), bf16),
            pltpu.VMEM((heads, dm, dm), bf16),
            pltpu.VMEM((heads, 8, lanes), f32),
            pltpu.VMEM((heads, 8, lanes), f32),
            pltpu.VMEM((rows, width + stick_width), bf16),
            pltpu.VMEM((rows, features), f32),
            pltpu.VMEM((n_out, half, features // n_out), bf16),
            pltpu.VMEM((n_out, half, features // n_out), bf16),
            dma((12,)),
            dma((1,)),
            dma((1,)),
            dma((1,)),
            dma((4,)),
            dma((1,)),
            dma((2,)),
            dma((2,)),
            dma((5,)),
            dma((2,)),
            dma((4,)),
            dma((1,)),
            dma((5,)),
            dma((n_sp - 1,)),
            dma((n_sp - 1,)),
            dma((2,)),
            dma((2,)),
            dma((1,)),
            dma((4 * heads,)),
            dma((1,)),
            dma((heads,)),
            dma((1,)),
            dma((n_out,)),
        ],
        compiler_params=pltpu.CompilerParams(
            collective_id=0, has_side_effects=True, vmem_limit_bytes=60 * 1024 * 1024
        ),
    )(
        tokens[0],
        norm_gain[None],
        memory_ingate.T,
        memory_forget.T,
        forget_bias,
        forget_shift[0].T,
        stick_bias,
        memory_gain[None],
        stick_gain[None],
        memory_key,
        memory_value,
        memory_query,
        memory_outgate,
        stick_query,
        stick_key,
        stick_value,
        out_memory,
        out_stick,
    )
    return out[None]


def solution(mesh):
    assert mesh.shape["fs"] == 4 and mesh.shape["tp"] == 2
    return jax.shard_map(
        functools.partial(per_device, mesh.shape["sp"]),
        mesh=mesh,
        in_specs=(
            P("fs", "sp", "tp"),
            P(),
            P("fs", "tp"),
            P("fs", "tp"),
            P("fs", "tp"),
            P("fs", "tp"),
            P(None, "tp"),
            P(None, "tp"),
            P("tp"),
            P("fs", "sp", "tp"),
            P(None, "tp"),
            P(None, "tp"),
            P(None, "tp"),
            P("tp"),
            P("tp"),
            P("tp"),
            P("tp", None),
            P("tp", None),
        ),
        out_specs=P("fs", ("sp", "tp"), None),
        check_vma=False,
    )
```

```python
import functools

import jax
import jax.numpy as jnp
from jax import lax
from jax.experimental import pallas as pl
from jax.experimental.pallas import tpu as pltpu
from jax.sharding import PartitionSpec as P

MESH = pl.DeviceIdType.MESH
epsilon = 1e-06
floor_neg = -1e30
f32 = jnp.float32
bf16 = jnp.bfloat16

KEY, VALUE, QUERY, GATE = 0, 1, 2, 3


def dot(a, b, dims=((1,), (0,))):
    return lax.dot_general(a, b, (dims, ((), ())), preferred_element_type=f32)


def softplus(z):
    return jnp.maximum(z, 0.0) + jnp.log(1.0 + jnp.exp(-jnp.abs(z)))


def kernel(
    n_sp,
    n_out,
    tok_hbm,
    gain_hbm,
    ingate_hbm,
    forget_hbm,
    bias_hbm,
    shift_hbm,
    sbias_hbm,
    mgain_hbm,
    sgain_hbm,
    wk_hbm,
    wv_hbm,
    wq_hbm,
    wo_hbm,
    sq_hbm,
    sk_hbm,
    sv_hbm,
    om_hbm,
    os_hbm,
    out_ref,
    tok_ref,
    gain_ref,
    ingate_ref,
    forget_ref,
    shift_ref,
    bias_ref,
    sbias_ref,
    mgain_ref,
    sgain_ref,
    tok_in,
    nrm,
    xg,
    wm,
    wg,
    ws,
    wout,
    sb,
    rb,
    own_part,
    proj,
    queries,
    kv,
    stick_acc,
    stick_run,
    far_out,
    far_in,
    gw,
    u_rows,
    u_cols,
    totals,
    tops,
    state_own,
    state_in,
    state_out,
    log_in,
    log_out,
    mix,
    early_out,
    ob,
    orb,
    load_sem,
    tok_s,
    tok_r,
    a2a_s,
    a2a_r,
    fwd_s,
    fwd_r,
    w_s,
    w_r,
    pass_s,
    z_r,
    rs_s,
    rs_r,
    kv_s,
    kv_r,
    far_s,
    far_r,
    chain_s,
    chain_r,
    log_s,
    log_r,
    out_s,
    out_r,
):
    f = lax.axis_index("fs")
    s = lax.axis_index("sp")
    t = lax.axis_index("tp")
    rows, half_feat = tok_ref.shape
    heads = state_own.shape[0]
    dm = state_own.shape[1]
    ds = sgain_ref.shape[1] // heads
    block = wm.shape[1]
    half = rows // 2
    other = 1 - t
    last = n_sp - 1
    helper = n_sp - 2

    def flip(bits):
        if bits == 1:
            return f + 1 - 2 * (f % 2)
        if bits == 2:
            return f + 2 - 4 * (f // 2)
        return 3 - f

    def remote(src, dst, send, recv, device):
        return pltpu.make_async_remote_copy(
            src_ref=src,
            dst_ref=dst,
            send_sem=send,
            recv_sem=recv,
            device_id=device,
            device_id_type=MESH,
        )

    barrier = pltpu.get_barrier_semaphore()
    pl.semaphore_signal(barrier, inc=1, device_id={"tp": other}, device_id_type=MESH)
    for bits in (1, 2):
        pl.semaphore_signal(barrier, inc=1, device_id={"fs": flip(bits)}, device_id_type=MESH)

    @pl.when(s > 0)
    def _():
        pl.semaphore_signal(barrier, inc=1, device_id={"sp": s - 1}, device_id_type=MESH)

    @pl.when(s < last)
    def _():
        pl.semaphore_signal(barrier, inc=1, device_id={"sp": s + 1}, device_id_type=MESH)

    def load(src, dst, at):
        return pltpu.make_async_copy(src, dst, load_sem.at[at])

    load(tok_hbm, tok_ref, 0).start()
    load(wk_hbm, wm.at[KEY], 1).start()
    load(wv_hbm, wm.at[VALUE], 1).start()
    load(gain_hbm, gain_ref, 2).start()
    load(sq_hbm, ws.at[0], 3).start()
    load(wq_hbm, wm.at[QUERY], 4).start()
    load(wo_hbm, wm.at[GATE], 4).start()
    load(sk_hbm, ws.at[1], 5).start()
    load(sv_hbm, ws.at[2], 5).start()
    load(ingate_hbm, ingate_ref, 6).start()
    load(forget_hbm, forget_ref, 7).start()
    load(shift_hbm, shift_ref, 8).start()
    load(bias_hbm, bias_ref, 12).start()
    load(sbias_hbm, sbias_ref, 13).start()
    load(om_hbm, wout.at[pl.ds(0, heads * dm)], 9).start()
    load(os_hbm, wout.at[pl.ds(heads * dm, heads * ds)], 9).start()
    load(mgain_hbm, mgain_ref, 10).start()
    load(sgain_hbm, sgain_ref, 11).start()

    def loaded(ref, at):
        pltpu.make_async_copy(ref, ref, load_sem.at[at]).wait()

    peers = 3 + jnp.where(s > 0, 1, 0) + jnp.where(s < last, 1, 0)
    pl.semaphore_wait(barrier, peers)

    loaded(tok_ref, 0)
    tok_copy = remote(tok_ref, tok_in, tok_s.at[0], tok_r.at[0], {"tp": other})

    def role(p, h):
        return (p + h) % 2

    def pair_bits(p, h):
        return 1 + role(p, h)

    def sum_bits(p, h):
        return 2 - role(p, h)

    first, second = [(KEY, 0), (VALUE, 0)], [(KEY, 1), (VALUE, 1)]
    third, fourth = [(QUERY, h) for h in range(heads)], [(GATE, h) for h in range(heads)]
    def part(number, count, parts=1, offset=0):
        size = block // count
        return pl.ds(pl.multiple_of(number * size, size) + offset * (size // parts), size // parts)

    parity, rest = part(s % 2, 2), part(1 - s % 2, 2)
    splits = 4
    fourth_own, fourth_rest, fourth_all = part(s % 2, 4), part(1 - s % 2, 4), part(1, 2)

    def stage(p, h):
        return h if p < 2 else p

    def weight_copy(p, h, lines, at, sem):
        return remote(
            wm.at[p, lines, pl.ds(h * dm, dm)], wg.at[p, h, lines], w_s.at[sem],
            w_r.at[at], {"fs": flip(pair_bits(p, h))},
        )

    def pass_copy(p, h, lines, at, to):
        return remote(
            wg.at[p, h, lines], wg.at[p, h, lines], pass_s.at[at], z_r.at[stage(p, h)], {"sp": to}
        )

    def both(p, h, lines):
        return wg.at[pl.ds(0, 2), h, lines] if p < 2 else wg.at[p, :, lines]

    def await_bytes(ref, sem):
        remote(ref, ref, pass_s.at[0], sem, {"tp": other}).wait_recv()

    def sent_bytes(ref, sem):
        remote(ref, ref, sem, z_r.at[0], {"tp": other}).wait_send()

    def send_weights(items, lines, at, sem=0):
        for p, h in items:
            weight_copy(p, h, lines, at, sem).start()

    def pass_weights(items, lines, at, sem=0):
        p, h = items[0]
        await_bytes(both(p, h, lines), w_r.at[at])
        down = (s > 0) & (s < last) if items is fourth else s > 0
        for p, h in items:
            @pl.when(down)
            def _():
                pass_copy(p, h, lines, sem, s - 1).start()

            @pl.when(s == helper)
            def _():
                pass_copy(p, h, lines, 2 + sem, s + 1).start()

    def first_lines(c):
        return part(s % 2, 2, splits, c)

    def rest_weights(items):
        p, h = items[0]
        if items is not fourth:
            await_bytes(both(p, h, rest), z_r.at[stage(p, h)])
            return
        await_bytes(both(p, h, fourth_all), w_r.at[splits + 3])

        @pl.when(s != helper)
        def _():
            await_bytes(both(p, h, fourth_rest), z_r.at[stage(p, h)])

        @pl.when(s == helper)
        def _():
            await_bytes(both(p, h, fourth_rest), w_r.at[splits + 4])

    def on_core(where, step):
        @pl.when(t == where)
        def _():
            step()

    on_core(1, tok_copy.start)
    loaded(wm.at[pl.ds(KEY, 2)], 1)
    for c in range(splits):
        send_weights(first, first_lines(c), c)
    send_weights(second, parity, splits)
    on_core(0, tok_copy.start)
    tok_copy.wait_recv()
    loaded(gain_ref, 2)

    step_rows = 32
    own_cols = pl.ds(pl.multiple_of(t * half_feat, half_feat), half_feat)
    far_cols = pl.ds(pl.multiple_of(other * half_feat, half_feat), half_feat)

    def norm_rows(i, _):
        at = pl.ds(pl.multiple_of(i * step_rows, step_rows), step_rows)
        own = tok_ref[at, :].astype(f32)
        far = tok_in[at, :].astype(f32)
        total = jnp.sum(own * own, axis=1, keepdims=True) + jnp.sum(far * far, axis=1, keepdims=True)
        scale = lax.rsqrt(total / (2 * half_feat) + epsilon)
        nrm[at, own_cols] = (own * scale * gain_ref[:, own_cols]).astype(bf16)
        nrm[at, far_cols] = (far * scale * gain_ref[:, far_cols]).astype(bf16)
        return 0

    lax.fori_loop(0, rows // step_rows, norm_rows, 0)

    my_rows = pl.ds(pl.multiple_of(t * half, half), half)
    cut = rows * 7 // 16
    core_rows = (pl.ds(0, cut), pl.ds(cut, rows - cut))

    def feature_block(index):
        return pl.ds(pl.multiple_of(index * block, block), block)

    def a2a_copy(core, r, which):
        lines = core_rows[core]
        to = flip(2 - r)
        return remote(
            nrm.at[lines, feature_block(to if which == 0 else flip(3))],
            xg.at[r, which, lines],
            a2a_s.at[0],
            a2a_r.at[r * 2 + which],
            {"fs": to},
        )

    def fwd_copy(core, r, which):
        lines = core_rows[core]
        return remote(
            xg.at[r, which, lines], xg.at[r, which, lines], fwd_s.at[0], fwd_r.at[r], {"tp": other}
        )

    def a2a_start(core):
        for r in range(2):
            for which in range(2):
                a2a_copy(core, r, which).start()

    on_core(0, lambda: a2a_start(0))
    on_core(1, lambda: a2a_start(1))
    loaded(wm.at[pl.ds(QUERY, 2)], 4)
    on_core(0, lambda: send_weights(third, parity, splits + 1))
    loaded(ws.at[0], 3)
    normed = nrm[...]
    queries[0] = dot(normed, ws[0]).astype(bf16)

    def query_copy():
        return remote(queries.at[0], queries.at[1], far_s.at[0], far_r.at[0], {"sp": s - 1})

    def kv_copy(d):
        return remote(kv.at[d - 1], kv.at[d], kv_s.at[d], kv_r.at[d], {"sp": s + 1})

    def kv_send(d):
        @pl.when((s < helper) & (s >= d - 1))
        def _():
            kv_copy(d).start()

    def kv_project():
        loaded(ws.at[pl.ds(1, 2)], 5)
        normed = nrm[...]
        kv[0, 0] = dot(normed, ws[1]).astype(bf16)
        kv[0, 1] = dot(normed, ws[2]).astype(bf16)
        kv_send(1)

    def pass_first():
        for c in range(splits):
            pass_weights(first, first_lines(c), c)

    on_core(0, kv_project)
    pass_first()
    on_core(1, kv_project)

    row_at = lax.broadcasted_iota(jnp.int32, (rows, rows), 0)
    col_at = lax.broadcasted_iota(jnp.int32, (rows, rows), 1)
    loaded(ingate_ref, 6)
    loaded(forget_ref, 7)
    loaded(shift_ref, 8)
    load(bias_hbm, bias_ref, 12).wait()
    load(sbias_hbm, sbias_ref, 13).wait()
    gw[...] = jnp.zeros(gw.shape, bf16)
    gw[0:heads, :] = ingate_ref[...]
    gw[8 : 8 + heads, :] = forget_ref[...]
    gate = dot(gw[...], normed, ((1,), (1,)))
    triu = (row_at <= col_at).astype(f32)
    u_rows[...] = jnp.zeros(u_rows.shape, f32)
    for h in range(heads):
        log_forget = shift_ref[h : h + 1, :] - softplus(-(gate[8 + h : 9 + h, :] + bias_ref[0:1, h : h + 1]))
        cumulative = lax.dot_general(
            jnp.broadcast_to(log_forget, (8, rows)), triu, (((1,), (0,)), ((), ())),
            precision=lax.Precision.HIGHEST, preferred_element_type=f32,
        )
        u_rows[h : h + 1, :] = gate[h : h + 1, :] - cumulative[0:1, :]
        totals[h : h + 1, :] = jnp.broadcast_to(
            cumulative[0:1, rows - 1 : rows], (1, totals.shape[1])
        )
    u_cols[...] = jnp.transpose(u_rows[...])

    pass_weights(second, parity, splits)

    @pl.when(s == last)
    def _():
        query_copy().start()


    def stick_part(at, h, kv_at, diagonal):
        cols = slice(h * ds, (h + 1) * ds)
        z = dot(queries[at, :, cols], kv[kv_at, 0, :, cols], ((1,), (1,)))
        z = z * ds ** (-0.5) + sbias_ref[0:1, h : h + 1]
        keep = -softplus(z)
        visible = col_at < row_at
        if diagonal:
            kept = jnp.where(visible, keep, 0.0)
        else:
            kept = keep
        strict = (row_at > col_at).astype(bf16)
        high = kept.astype(bf16)
        low = (kept - high.astype(f32)).astype(bf16)
        after = dot(high, strict) + dot(low, strict)
        weights = jnp.exp(z + keep + after)
        if diagonal:
            weights = jnp.where(visible, weights, 0.0)
        part = dot(weights.astype(bf16), kv[kv_at, 1, :, cols])
        return part, jnp.sum(kept, axis=1, keepdims=True)

    def stick_first(at, diagonal):
        for h in range(heads):
            part, keep = stick_part(at, h, 0, diagonal)
            stick_acc[at, h] = part
            stick_run[at, h] = jnp.broadcast_to(keep, stick_run.shape[2:])

    def kv_forward(d):
        @pl.when((s >= d) & (s <= helper))
        def _():
            remote(kv.at[d - 1], kv.at[d], kv_s.at[d], kv_r.at[d], {"sp": s - 1}).wait_recv()

        @pl.when((s >= d) & (s < helper))
        def _():
            kv_copy(d + 1).start()

    def stick_span(at, d):
        for h in range(heads):
            part, keep = stick_part(at, h, d, False)
            stick_acc[at, h] = stick_acc[at, h] + jnp.exp(stick_run[at, h]) * part
            stick_run[at, h] = stick_run[at, h] + keep

    def own_span(d):
        @pl.when((s >= d) & (s <= helper))
        def _():
            stick_span(0, d)

    def far_span(d):
        @pl.when(s == helper)
        def _():
            stick_span(1, d)

    def over(low, high, step):
        if high > low:
            lax.fori_loop(low, high, lambda d, c: (step(d), c)[1], 0)

    stick_first(0, True)

    def a2a_forward(core):
        for which in range(2):
            for r in range(2):
                a2a_copy(core, r, which).wait_recv()
                fwd_copy(core, r, which).start()

    on_core(0, lambda: a2a_forward(0))
    on_core(1, lambda: a2a_forward(1))
    on_core(1, lambda: send_weights(third, parity, splits + 1))
    far_rows = pl.ds(pl.multiple_of(other * half, half), half)

    def rs_sem(p, h):
        return h if p < 2 else p + (h if p == GATE else 0)

    def rs_copy(p, h, lines):
        return remote(
            sb.at[p, h, lines], rb.at[p, h, lines], rs_s.at[0], rs_r.at[rs_sem(p, h)],
            {"fs": flip(sum_bits(p, h))},
        )

    def partials(items):
        rest_weights(items)
        for p, h in items:
            cols = slice(h * dm, (h + 1) * dm)
            r = role(p, h)
            sb[p, h] = (dot(xg[r, 0], wm[p, :, cols]) + dot(xg[r, 1], wg[p, h])).astype(bf16)
            rs_copy(p, h, pl.ds(0, rows)).start()

    def first_partials(items, core):
        for at in (core, 1 - core):
            lines = core_rows[at]
            for p, h in items:
                cols = slice(h * dm, (h + 1) * dm)
                r = role(p, h)
                if at != core:
                    await_bytes(xg.at[r, :, lines], fwd_r.at[r])
                sb[p, h, lines] = (
                    dot(xg[r, 0, lines], wm[p, :, cols]) + dot(xg[r, 1, lines], wg[p, h])
                ).astype(bf16)
                rs_copy(p, h, lines).start()

    def own_partials(items):
        for p, h in items:
            cols = slice(h * dm, (h + 1) * dm)
            own_part[p, h] = dot(nrm[:, feature_block(f)], wm[p, :, cols]) + dot(
                nrm[:, feature_block(flip(pair_bits(p, h)))], wg[p, h]
            )

    def finish(p, h):
        return (own_part[p, h] + rb[p, h].astype(f32)).astype(bf16)

    def column(h):
        return u_cols[:, h : h + 1]

    def own_state(h):
        await_bytes(rb.at[pl.ds(0, 2), h], rs_r.at[h])
        proj[KEY, h] = (finish(KEY, h).astype(f32) * dm ** (-0.5)).astype(bf16)
        proj[VALUE, h] = finish(VALUE, h)
        u = column(h)
        top = jnp.max(u, axis=0, keepdims=True)
        weighted = (proj[KEY, h].astype(f32) * jnp.exp(u - top)).astype(bf16)
        state_own[h] = dot(weighted, proj[VALUE, h], ((0,), (0,)))

    def log_copy(h, to):
        return remote(log_out.at[h], log_in.at[h], log_s.at[0], log_r.at[h], {"sp": to})

    piece_dm = dm // 2
    pieces = 4

    def chain_copy(h, c, to):
        lines = pl.ds(c // 2 * piece_dm, piece_dm)
        cols = pl.ds(c % 2 * piece_dm, piece_dm)
        at = h * pieces + c
        return remote(
            state_out.at[h, lines, cols], state_in.at[h, lines, cols], chain_s.at[0], chain_r.at[at],
            {"sp": to},
        )

    def chain(h):
        @pl.when(s == 0)
        def _():
            log_in[h] = jnp.full(log_in.shape[1:], floor_neg, f32)
            state_in[h] = jnp.zeros(state_in.shape[1:], bf16)

        @pl.when(s > 0)
        def _():
            log_copy(h, s - 1).wait_recv()

        total = totals[h : h + 1, 0:1]
        early = total + log_in[h, 0:1, 0:1]
        late = total + jnp.max(column(h), axis=0, keepdims=True)
        top = jnp.maximum(early, late)

        @pl.when(s < last)
        def _():
            log_out[h] = jnp.broadcast_to(top, log_out.shape[1:])
            log_copy(h, s + 1).start()

        early, late = jnp.exp(early - top), jnp.exp(late - top)
        for c in range(pieces):
            lines = pl.ds(c // 2 * piece_dm, piece_dm)
            cols = pl.ds(c % 2 * piece_dm, piece_dm)

            @pl.when(s > 0)
            def _():
                chain_copy(h, c, s - 1).wait_recv()

            @pl.when(s < last)
            def _():
                state_out[h, lines, cols] = (
                    early * state_in[h, lines, cols].astype(f32) + late * state_own[h, lines, cols]
                ).astype(bf16)
                chain_copy(h, c, s + 1).start()

    def chain_if(where, h):
        @pl.when(where)
        def _():
            chain(h)

    over(1, min(2, n_sp - 1), kv_forward)
    rest_weights(first)
    on_core(0, lambda: first_partials(first, 0))
    on_core(1, lambda: first_partials(first, 1))
    send_weights(fourth, fourth_own, splits + 2, 1)
    own_partials(first)
    pass_weights(third, parity, splits + 1)
    over(1, min(2, n_sp - 1), own_span)
    partials(second)
    send_weights(fourth, fourth_all, splits + 3, 2)

    @pl.when(s == helper)
    def _():
        send_weights(fourth, fourth_rest, splits + 4, 3)

    own_partials(second)
    own_state(0)
    chain_if(s == 0, 0)
    pass_weights(fourth, fourth_own, splits + 2, 1)
    @pl.when(s == helper)
    def _():
        query_copy().wait_recv()
        stick_first(1, False)

    over(1, min(2, n_sp - 1), far_span)
    over(2, n_sp - 1, kv_forward)
    over(2, n_sp - 1, own_span)
    over(2, n_sp - 1, far_span)

    @pl.when(s == helper)
    def _():
        far_out[...] = stick_acc[1].astype(bf16)
        remote(far_out, far_in, far_s.at[1], far_r.at[1], {"sp": s + 1}).start()

    own_state(1)
    chain_if(s == 0, 1)
    chain_if(s == 1, 0)
    partials(third)
    chain_if(s == 2, 0)
    own_partials(third)
    partials(fourth)
    chain_if(s == 1, 1)
    own_partials(fourth)
    loaded(wout, 9)
    loaded(mgain_ref, 10)
    loaded(sgain_ref, 11)
    chain_if(s == 2, 1)

    causal = col_at <= row_at
    await_bytes(rb.at[QUERY], rs_r.at[QUERY])
    for h in range(heads):
        proj[QUERY, h] = finish(QUERY, h)
        masked = jnp.where(causal, u_rows[h : h + 1, :], floor_neg)
        top = jnp.max(masked, axis=1, keepdims=True)
        scores = dot(proj[QUERY, h], proj[KEY, h], ((1,), (1,))) * jnp.exp(masked - top)
        own_part[QUERY, h] = dot(scores.astype(bf16), proj[VALUE, h])
        tops[h] = jnp.broadcast_to(top, tops.shape[1:])

    @pl.when(s == last)
    def _():
        remote(far_out, far_in, far_s.at[1], far_r.at[1], {"sp": s - 1}).wait_recv()
        for h in range(heads):
            stick_acc[0, h] = stick_acc[0, h] + jnp.exp(stick_run[0, h]) * far_in[h].astype(f32)

    for h in range(heads):
        cols = slice(h * ds, (h + 1) * ds)
        out = stick_acc[0, h]
        scale = lax.rsqrt(jnp.mean(out * out, axis=1, keepdims=True) + epsilon)
        mix[:, heads * dm + h * ds : heads * dm + (h + 1) * ds] = (
            out * scale * sgain_ref[:, cols]
        ).astype(bf16)
    early_out[...] = dot(mix[:, heads * dm :], wout[heads * dm :, :])

    for h in range(heads):
        chain_if(s > 2, h)
        carried_max = log_in[h, 0:1, 0:1]
        top = tops[h, :, 0:1]
        running = jnp.maximum(carried_max, top)
        own_part[QUERY, h] = jnp.exp(top - running) * own_part[QUERY, h] + jnp.exp(
            carried_max - running
        ) * dot(proj[QUERY, h], state_in[h])
        await_bytes(rb.at[GATE, h], rs_r.at[GATE + h])
        gated = own_part[QUERY, h] / (1.0 + jnp.exp(-finish(GATE, h).astype(f32)))
        scale = lax.rsqrt(jnp.mean(gated * gated, axis=1, keepdims=True) + epsilon)
        cols = slice(h * dm, (h + 1) * dm)
        mix[:, cols] = (gated * scale * mgain_ref[:, cols]).astype(bf16)
        if h < heads - 1:
            early_out[...] = early_out[...] + dot(mix[:, cols], wout[cols, :])

    piece = wout.shape[1] // n_out
    lines = slice((heads - 1) * dm, heads * dm)
    copies = []
    for c in range(n_out):
        cols = slice(c * piece, (c + 1) * piece)
        ob[c] = (early_out[far_rows, cols] + dot(mix[far_rows, lines], wout[lines, cols])).astype(bf16)
        copy = remote(ob.at[c], orb.at[c], out_s.at[0], out_r.at[c], {"tp": other})
        copy.start()
        copies.append(copy)
    for c in range(n_out):
        cols = slice(c * piece, (c + 1) * piece)
        early_out[my_rows, cols] = early_out[my_rows, cols] + dot(mix[my_rows, lines], wout[lines, cols])
    for c in range(n_out):
        cols = slice(c * piece, (c + 1) * piece)
        copies[c].wait_recv()
        out_ref[:, cols] = (early_out[my_rows, cols] + orb[c].astype(f32)).astype(bf16)

    tok_copy.wait_send()

    def a2a_sent(core):
        sent_bytes(xg.at[:, :, core_rows[core]], a2a_s.at[0])
        sent_bytes(xg.at[:, :, core_rows[core]], fwd_s.at[0])

    on_core(0, lambda: a2a_sent(0))
    on_core(1, lambda: a2a_sent(1))
    sent_bytes(wm.at[pl.ds(0, 3), parity], w_s.at[0])
    sent_bytes(wm.at[GATE, fourth_own], w_s.at[1])
    sent_bytes(wm.at[GATE, fourth_all], w_s.at[2])
    sent_bytes(sb, rs_s.at[0])
    sent_bytes(ob, out_s.at[0])

    @pl.when(s > 0)
    def _():
        sent_bytes(wg.at[pl.ds(0, 3), :, parity], pass_s.at[0])

    @pl.when((s > 0) & (s < last))
    def _():
        sent_bytes(wg.at[GATE, :, fourth_own], pass_s.at[1])

    @pl.when(s == helper)
    def _():
        sent_bytes(wg.at[pl.ds(0, 3), :, parity], pass_s.at[2])
        sent_bytes(wg.at[GATE, :, fourth_own], pass_s.at[3])
        sent_bytes(wm.at[GATE, fourth_rest], w_s.at[3])
        remote(far_out, far_in, far_s.at[1], far_r.at[1], {"sp": s + 1}).wait_send()

    @pl.when(s == last)
    def _():
        query_copy().wait_send()

    @pl.when(s < last)
    def _():
        sent_bytes(log_out, log_s.at[0])
        sent_bytes(state_out, chain_s.at[0])

    def kv_done(d, c):
        @pl.when((s < helper) & (s >= d - 1))
        def _():
            kv_copy(d).wait_send()

        return c

    lax.fori_loop(1, n_sp - 1, kv_done, 0)


def per_device(
    n_sp,
    tokens,
    norm_gain,
    memory_query,
    memory_key,
    memory_value,
    memory_outgate,
    memory_ingate,
    memory_forget,
    forget_bias,
    forget_shift,
    stick_query,
    stick_key,
    stick_value,
    stick_bias,
    memory_gain,
    stick_gain,
    out_memory,
    out_stick,
):
    rows, half_feat = tokens.shape[1:]
    features = 2 * half_feat
    heads = forget_bias.shape[0]
    block, width = memory_query.shape
    dm = width // heads
    stick_width = stick_query.shape[1]
    ds = stick_width // heads
    lanes = 128
    n_out = 4
    half = rows // 2

    vmem = pl.BlockSpec(memory_space=pltpu.VMEM)
    anyw = pl.BlockSpec(memory_space=pl.ANY)
    dma = pltpu.SemaphoreType.DMA
    out = pl.pallas_call(
        functools.partial(kernel, n_sp, n_out),
        out_shape=pltpu.VMEM((half, features), bf16),
        in_specs=[anyw] * 18,
        out_specs=vmem,
        scratch_shapes=[
            pltpu.VMEM((rows, half_feat), bf16),
            pltpu.VMEM((1, features), f32),
            pltpu.VMEM((heads, features), bf16),
            pltpu.VMEM((heads, features), bf16),
            pltpu.VMEM((heads, rows), f32),
            pltpu.VMEM((1, heads), f32),
            pltpu.VMEM((1, heads), f32),
            pltpu.VMEM((1, width), f32),
            pltpu.VMEM((1, stick_width), f32),
            pltpu.VMEM((rows, half_feat), bf16),
            pltpu.VMEM((rows, features), bf16),
            pltpu.VMEM((2, 2, rows, block), bf16),
            pltpu.VMEM((4, block, width), bf16),
            pltpu.VMEM((4, heads, block, dm), bf16),
            pltpu.VMEM((3, features, stick_width), bf16),
            pltpu.VMEM((width + stick_width, features), bf16),
            pltpu.VMEM((4, heads, rows, dm), bf16),
            pltpu.VMEM((4, heads, rows, dm), bf16),
            pltpu.VMEM((4, heads, rows, dm), f32),
            pltpu.VMEM((4, heads, rows, dm), bf16),
            pltpu.VMEM((2, rows, stick_width), bf16),
            pltpu.VMEM((n_sp - 1, 2, rows, stick_width), bf16),
            pltpu.VMEM((2, heads, rows, ds), f32),
            pltpu.VMEM((2, heads, rows, ds), f32),
            pltpu.VMEM((heads, rows, ds), bf16),
            pltpu.VMEM((heads, rows, ds), bf16),
            pltpu.VMEM((16, features), bf16),
            pltpu.VMEM((lanes, rows), f32),
            pltpu.VMEM((rows, lanes), f32),
            pltpu.VMEM((8, lanes), f32),
            pltpu.VMEM((heads, rows, lanes), f32),
            pltpu.VMEM((heads, dm, dm), f32),
            pltpu.VMEM((heads, dm, dm), bf16),
            pltpu.VMEM((heads, dm, dm), bf16),
            pltpu.VMEM((heads, 8, lanes), f32),
            pltpu.VMEM((heads, 8, lanes), f32),
            pltpu.VMEM((rows, width + stick_width), bf16),
            pltpu.VMEM((rows, features), f32),
            pltpu.VMEM((n_out, half, features // n_out), bf16),
            pltpu.VMEM((n_out, half, features // n_out), bf16),
            dma((14,)),
            dma((1,)),
            dma((1,)),
            dma((1,)),
            dma((4,)),
            dma((1,)),
            dma((2,)),
            dma((4,)),
            dma((9,)),
            dma((4,)),
            dma((4,)),
            dma((1,)),
            dma((5,)),
            dma((n_sp - 1,)),
            dma((n_sp - 1,)),
            dma((2,)),
            dma((2,)),
            dma((1,)),
            dma((4 * heads,)),
            dma((1,)),
            dma((heads,)),
            dma((1,)),
            dma((n_out,)),
        ],
        compiler_params=pltpu.CompilerParams(
            collective_id=0, has_side_effects=True, vmem_limit_bytes=60 * 1024 * 1024
        ),
    )(
        tokens[0],
        norm_gain[None],
        memory_ingate.T,
        memory_forget.T,
        forget_bias[None],
        forget_shift[0].T,
        stick_bias[None],
        memory_gain[None],
        stick_gain[None],
        memory_key,
        memory_value,
        memory_query,
        memory_outgate,
        stick_query,
        stick_key,
        stick_value,
        out_memory,
        out_stick,
    )
    return out[None]


def solution(mesh):
    assert mesh.shape["fs"] == 4 and mesh.shape["tp"] == 2
    return jax.shard_map(
        functools.partial(per_device, mesh.shape["sp"]),
        mesh=mesh,
        in_specs=(
            P("fs", "sp", "tp"),
            P(),
            P("fs", "tp"),
            P("fs", "tp"),
            P("fs", "tp"),
            P("fs", "tp"),
            P(None, "tp"),
            P(None, "tp"),
            P("tp"),
            P("fs", "sp", "tp"),
            P(None, "tp"),
            P(None, "tp"),
            P(None, "tp"),
            P("tp"),
            P("tp"),
            P("tp"),
            P("tp", None),
            P("tp", None),
        ),
        out_specs=P("fs", ("sp", "tp"), None),
        check_vma=False,
    )
```

```python
import functools

import jax
import jax.numpy as jnp
from jax import lax
from jax.experimental import pallas as pl
from jax.experimental.pallas import tpu as pltpu
from jax.sharding import PartitionSpec as P

MESH = pl.DeviceIdType.MESH
epsilon = 1e-06
floor_neg = -1e30
f32 = jnp.float32
bf16 = jnp.bfloat16

KEY, VALUE, QUERY, GATE = 0, 1, 2, 3


def dot(a, b, dims=((1,), (0,))):
    return lax.dot_general(a, b, (dims, ((), ())), preferred_element_type=f32)


def softplus(z):
    return jnp.maximum(z, 0.0) + jnp.log(1.0 + jnp.exp(-jnp.abs(z)))


def kernel(
    n_sp,
    tok_hbm,
    gain_hbm,
    ingate_hbm,
    forget_hbm,
    bias_hbm,
    shift_hbm,
    sbias_hbm,
    mgain_hbm,
    sgain_hbm,
    wk_hbm,
    wv_hbm,
    wq_hbm,
    wo_hbm,
    sq_hbm,
    sk_hbm,
    sv_hbm,
    om_hbm,
    os_hbm,
    out_ref,
    tok_ref,
    gain_ref,
    gate_in,
    shift_ref,
    bias_ref,
    sbias_ref,
    gains,
    tok_in,
    nrm,
    xg,
    wm,
    wg,
    ws,
    wout,
    sb,
    rb,
    own_part,
    proj,
    queries,
    kv,
    stick_acc,
    stick_run,
    far_out,
    far_in,
    gw,
    u_rows,
    u_cols,
    totals,
    tops,
    state_own,
    state_in,
    state_out,
    log_in,
    log_out,
    factors,
    mix,
    mix_in,
    wout_in,
    early_out,
    load_sem,
    send_s,
    tok_r,
    a2a_r,
    fwd_r,
    w_r,
    z_r,
    rs_r,
    kv_s,
    kv_r,
    far_s,
    far_r,
    chain_s,
    chain_r,
    log_s,
    log_r,
    out_r,
):
    f = lax.axis_index("fs")
    s = lax.axis_index("sp")
    t = lax.axis_index("tp")
    rows, half_feat = tok_ref.shape
    features = wout.shape[1]
    heads = state_own.shape[0]
    dm = state_own.shape[1]
    ds = stick_acc.shape[3]
    block = wm.shape[1]
    half = rows // 2
    other = 1 - t
    last = n_sp - 1
    helper = n_sp - 2

    def flip(bits):
        if bits == 1:
            return f + 1 - 2 * (f % 2)
        if bits == 2:
            return f + 2 - 4 * (f // 2)
        return 3 - f

    def remote(src, dst, send, recv, device):
        return pltpu.make_async_remote_copy(
            src_ref=src,
            dst_ref=dst,
            send_sem=send,
            recv_sem=recv,
            device_id=device,
            device_id_type=MESH,
        )

    barrier = pltpu.get_barrier_semaphore()
    pl.semaphore_signal(barrier, inc=1, device_id={"tp": other}, device_id_type=MESH)
    for bits in (1, 2):
        pl.semaphore_signal(barrier, inc=1, device_id={"fs": flip(bits)}, device_id_type=MESH)

    @pl.when(s > 0)
    def _():
        pl.semaphore_signal(barrier, inc=1, device_id={"sp": s - 1}, device_id_type=MESH)

    @pl.when(s < last)
    def _():
        pl.semaphore_signal(barrier, inc=1, device_id={"sp": s + 1}, device_id_type=MESH)

    def load(src, dst, at):
        return pltpu.make_async_copy(src, dst, load_sem.at[at])

    load(tok_hbm, tok_ref, 0).start()
    load(wk_hbm, wm.at[KEY], 1).start()
    load(wv_hbm, wm.at[VALUE], 1).start()
    load(gain_hbm, gain_ref, 2).start()
    load(sq_hbm, ws.at[0], 3).start()
    load(sk_hbm, ws.at[1], 3).start()
    load(sv_hbm, ws.at[2], 3).start()
    load(wq_hbm, wm.at[QUERY], 4).start()
    load(wo_hbm, wm.at[GATE], 4).start()
    load(ingate_hbm, gate_in.at[0], 5).start()
    load(forget_hbm, gate_in.at[1], 5).start()
    load(shift_hbm, shift_ref, 8).start()
    load(bias_hbm, bias_ref, 6).start()
    load(sbias_hbm, sbias_ref, 7).start()
    load(om_hbm, wout.at[pl.ds(0, heads * dm)], 9).start()
    load(os_hbm, wout.at[pl.ds(heads * dm, heads * ds)], 9).start()
    load(mgain_hbm, gains.at[:, pl.ds(0, heads * dm)], 10).start()
    load(sgain_hbm, gains.at[:, pl.ds(heads * dm, heads * ds)], 10).start()

    def loaded(ref, at):
        pltpu.make_async_copy(ref, ref, load_sem.at[at]).wait()

    peers = 3 + jnp.where(s > 0, 1, 0) + jnp.where(s < last, 1, 0)
    pl.semaphore_wait(barrier, peers)

    loaded(tok_ref, 0)
    tok_copy = remote(tok_ref, tok_in, send_s.at[2], tok_r.at[0], {"tp": other})

    def role(p, h):
        return (p + h) % 2

    def pair_bits(p, h):
        return 1 + role(p, h)

    def sum_bits(p, h):
        return 2 - role(p, h)

    first, second = [(KEY, 0), (VALUE, 0)], [(KEY, 1), (VALUE, 1)]
    third, fourth = [(QUERY, h) for h in range(heads)], [(GATE, h) for h in range(heads)]
    def part(number, count, parts=1, offset=0):
        size = block // count
        return pl.ds(pl.multiple_of(number * size, size) + offset * (size // parts), size // parts)

    parity, rest = part(s % 2, 2), part(1 - s % 2, 2)
    splits = 2
    fourth_own, fourth_rest, fourth_all = part(s % 2, 4), part(1 - s % 2, 4), part(1, 2)

    def stage(p, h):
        return h if p < 2 else p

    def weight_copy(p, h, lines, at):
        return remote(
            wm.at[p, lines, pl.ds(h * dm, dm)], wg.at[p, h, lines], send_s.at[0],
            w_r.at[at], {"fs": flip(pair_bits(p, h))},
        )

    def pass_copy(p, h, lines, at, to):
        return remote(
            wg.at[p, h, lines], wg.at[p, h, lines], send_s.at[1], z_r.at[stage(p, h)], {"sp": to}
        )

    def both(p, h, lines):
        return wg.at[pl.ds(0, 2), h, lines] if p < 2 else wg.at[p, :, lines]

    def await_bytes(ref, sem):
        remote(ref, ref, send_s.at[0], sem, {"tp": other}).wait_recv()

    def sent_bytes(ref, sem):
        remote(ref, ref, sem, z_r.at[0], {"tp": other}).wait_send()

    def send_weights(items, lines, at):
        for p, h in items:
            weight_copy(p, h, lines, at).start()

    def pass_weights(items, lines, at, sem=0):
        p, h = items[0]
        await_bytes(both(p, h, lines), w_r.at[at])
        down = (s > 0) & (s < last) if items is fourth else s > 0
        for p, h in items:
            @pl.when(down)
            def _():
                pass_copy(p, h, lines, sem, s - 1).start()

            if items is fourth:
                continue

            @pl.when(s == helper)
            def _():
                pass_copy(p, h, lines, 2 + sem, s + 1).start()

    def first_lines(c):
        return part(s % 2, 2, splits, c)

    def rest_weights(items):
        p, h = items[0]
        if items is not fourth:
            await_bytes(both(p, h, rest), z_r.at[stage(p, h)])
            return

        @pl.when(s < helper)
        def _():
            await_bytes(both(p, h, fourth_all), w_r.at[splits + 3])
            await_bytes(both(p, h, fourth_rest), z_r.at[stage(p, h)])

        @pl.when(s >= helper)
        def _():
            await_bytes(both(p, h, pl.ds(0, block - block // 4)), w_r.at[splits + 3])

    def on_core(where, step):
        @pl.when(t == where)
        def _():
            step()

    on_core(1, tok_copy.start)
    loaded(wm.at[pl.ds(KEY, 2)], 1)
    for c in range(splits):
        send_weights(first, first_lines(c), c)
    send_weights(second, parity, splits)
    on_core(0, tok_copy.start)
    tok_copy.wait_recv()
    loaded(gain_ref, 2)

    step_rows = 32
    own_cols = pl.ds(pl.multiple_of(t * half_feat, half_feat), half_feat)
    far_cols = pl.ds(pl.multiple_of(other * half_feat, half_feat), half_feat)

    def norm_rows(i, _):
        at = pl.ds(pl.multiple_of(i * step_rows, step_rows), step_rows)
        own = tok_ref[at, :].astype(f32)
        far = tok_in[at, :].astype(f32)
        total = jnp.sum(own * own, axis=1, keepdims=True) + jnp.sum(far * far, axis=1, keepdims=True)
        scale = lax.rsqrt(total / (2 * half_feat) + epsilon)
        nrm[at, own_cols] = (own * scale * gain_ref[:, own_cols]).astype(bf16)
        nrm[at, far_cols] = (far * scale * gain_ref[:, far_cols]).astype(bf16)
        return 0

    lax.fori_loop(0, rows // step_rows, norm_rows, 0)

    my_rows = pl.ds(pl.multiple_of(t * half, half), half)
    cut = rows * 7 // 16
    core_rows = (pl.ds(0, cut), pl.ds(cut, rows - cut))

    def feature_block(index):
        return pl.ds(pl.multiple_of(index * block, block), block)

    def a2a_copy(core, r, which):
        lines = core_rows[core]
        to = flip(2 - r)
        return remote(
            nrm.at[lines, feature_block(to if which == 0 else flip(3))],
            xg.at[r, which, lines],
            send_s.at[0],
            a2a_r.at[which],
            {"fs": to},
        )

    def fwd_copy(core, r, which):
        lines = core_rows[core]
        return remote(
            xg.at[r, which, lines], xg.at[r, which, lines], send_s.at[0], fwd_r.at[0], {"tp": other}
        )

    def a2a_start(core):
        for r in range(2):
            for which in range(2):
                a2a_copy(core, r, which).start()

    on_core(0, lambda: a2a_start(0))
    on_core(1, lambda: a2a_start(1))
    loaded(wm.at[pl.ds(QUERY, 2)], 4)
    send_weights(third, parity, splits + 1)
    loaded(ws, 3)
    normed = nrm[...]
    queries[0] = dot(normed, ws[0]).astype(bf16)

    def query_copy():
        return remote(queries.at[0], queries.at[1], far_s.at[0], far_r.at[0], {"sp": s - 1})

    def kv_copy(d):
        return remote(kv.at[d - 1], kv.at[d], kv_s.at[d - 1], kv_r.at[d - 1], {"sp": s + 1})

    def kv_send(d):
        @pl.when((s < helper) & (s >= d - 1))
        def _():
            kv_copy(d).start()

    def kv_project():
        normed = nrm[...]
        kv[0, 0] = dot(normed, ws[1]).astype(bf16)
        kv[0, 1] = dot(normed, ws[2]).astype(bf16)
        kv_send(1)

    def pass_first():
        for c in range(splits):
            pass_weights(first, first_lines(c), c)

    on_core(0, kv_project)
    pass_first()
    on_core(1, kv_project)

    row_at = lax.broadcasted_iota(jnp.int32, (rows, rows), 0)
    col_at = lax.broadcasted_iota(jnp.int32, (rows, rows), 1)
    loaded(gate_in, 5)
    loaded(shift_ref, 8)
    load(bias_hbm, bias_ref, 6).wait()
    load(sbias_hbm, sbias_ref, 7).wait()
    gw[...] = jnp.zeros(gw.shape, bf16)
    gw[0:heads, :] = gate_in[0]
    gw[8 : 8 + heads, :] = gate_in[1]
    gate = dot(gw[...], normed, ((1,), (1,)))
    triu = (row_at <= col_at).astype(f32)
    u_rows[...] = jnp.zeros(u_rows.shape, f32)
    for h in range(heads):
        log_forget = shift_ref[h : h + 1, :] - softplus(-(gate[8 + h : 9 + h, :] + bias_ref[0:1, h : h + 1]))
        cumulative = lax.dot_general(
            jnp.broadcast_to(log_forget, (8, rows)), triu, (((1,), (0,)), ((), ())),
            precision=lax.Precision.HIGHEST, preferred_element_type=f32,
        )
        u_rows[h : h + 1, :] = gate[h : h + 1, :] - cumulative[0:1, :]
        totals[h : h + 1, :] = jnp.broadcast_to(
            cumulative[0:1, rows - 1 : rows], (1, totals.shape[1])
        )
    u_cols[...] = jnp.transpose(u_rows[...])

    pass_weights(second, parity, splits)

    @pl.when(s == last)
    def _():
        query_copy().start()


    def stick_part(at, h, kv_at, diagonal):
        cols = slice(h * ds, (h + 1) * ds)
        z = dot(queries[at, :, cols], kv[kv_at, 0, :, cols], ((1,), (1,)))
        z = z * ds ** (-0.5) + sbias_ref[0:1, h : h + 1]
        keep = -softplus(z)
        visible = col_at < row_at
        if diagonal:
            kept = jnp.where(visible, keep, 0.0)
        else:
            kept = keep
        strict = (row_at > col_at).astype(bf16)
        high = kept.astype(bf16)
        low = (kept - high.astype(f32)).astype(bf16)
        after = dot(high, strict) + dot(low, strict)
        weights = jnp.exp(z + keep + after)
        if diagonal:
            weights = jnp.where(visible, weights, 0.0)
        part = dot(weights.astype(bf16), kv[kv_at, 1, :, cols])
        return part, after[:, 0:1] + kept[:, 0:1]

    def stick_first(at, diagonal):
        for h in range(heads):
            part, keep = stick_part(at, h, 0, diagonal)
            stick_acc[at, h] = part
            stick_run[at, h] = jnp.broadcast_to(keep, stick_run.shape[2:])

    def kv_forward(d):
        @pl.when((s >= d) & (s <= helper))
        def _():
            remote(kv.at[d - 1], kv.at[d], kv_s.at[d - 1], kv_r.at[d - 1], {"sp": s - 1}).wait_recv()

        @pl.when((s >= d) & (s < helper))
        def _():
            kv_copy(d + 1).start()

    def stick_span(at, d):
        for h in range(heads):
            part, keep = stick_part(at, h, d, False)
            stick_acc[at, h] = stick_acc[at, h] + jnp.exp(stick_run[at, h]) * part
            stick_run[at, h] = stick_run[at, h] + keep

    def own_span(d):
        @pl.when((s >= d) & (s <= helper))
        def _():
            stick_span(0, d)

    def far_span(d):
        @pl.when(s == helper)
        def _():
            stick_span(1, d)

    def over(low, high, step):
        if high > low:
            lax.fori_loop(low, high, lambda d, c: (step(d), c)[1], 0)

    loaded(wout, 9)
    wout_copy = remote(wout, wout_in, send_s.at[3], tok_r.at[1], {"tp": other})
    wout_copy.start()
    stick_first(0, True)

    def a2a_forward(core):
        for which in range(2):
            await_bytes(xg.at[:, which, core_rows[core]], a2a_r.at[which])
            for r in range(2):
                fwd_copy(core, r, which).start()

    on_core(0, lambda: a2a_forward(0))
    on_core(1, lambda: a2a_forward(1))
    far_rows = pl.ds(pl.multiple_of(other * half, half), half)

    def rs_sem(p, h):
        return h if p < 2 else p + (h if p == GATE else 0)

    def rs_copy(p, h, lines):
        return remote(
            sb.at[p, h, lines], rb.at[p, h, lines], send_s.at[1], rs_r.at[rs_sem(p, h)],
            {"fs": flip(sum_bits(p, h))},
        )

    def partials(items):
        rest_weights(items)
        for p, h in items:
            cols = slice(h * dm, (h + 1) * dm)
            r = role(p, h)
            sb[p, h] = (dot(xg[r, 0], wm[p, :, cols]) + dot(xg[r, 1], wg[p, h])).astype(bf16)
            rs_copy(p, h, pl.ds(0, rows)).start()

    def first_partials(items, core):
        for at in (core, 1 - core):
            lines = core_rows[at]
            if at != core:
                await_bytes(xg.at[:, :, lines], fwd_r.at[0])
            for p, h in items:
                cols = slice(h * dm, (h + 1) * dm)
                r = role(p, h)
                sb[p, h, lines] = (
                    dot(xg[r, 0, lines], wm[p, :, cols]) + dot(xg[r, 1, lines], wg[p, h])
                ).astype(bf16)
                rs_copy(p, h, lines).start()

    def own_partials(items):
        for p, h in items:
            cols = slice(h * dm, (h + 1) * dm)
            own_part[p, h] = dot(nrm[:, feature_block(f)], wm[p, :, cols]) + dot(
                nrm[:, feature_block(flip(pair_bits(p, h)))], wg[p, h]
            )

    def finish(p, h):
        return (own_part[p, h] + rb[p, h].astype(f32)).astype(bf16)

    def column(h):
        return u_cols[:, h : h + 1]

    def own_state(h):
        await_bytes(rb.at[pl.ds(0, 2), h], rs_r.at[h])
        proj[KEY, h] = (finish(KEY, h).astype(f32) * dm ** (-0.5)).astype(bf16)
        proj[VALUE, h] = finish(VALUE, h)
        u = column(h)
        top = jnp.max(u, axis=0, keepdims=True)
        weighted = (proj[KEY, h].astype(f32) * jnp.exp(u - top)).astype(bf16)
        state_own[h] = dot(weighted, proj[VALUE, h], ((0,), (0,)))

    def log_copy(h, to):
        return remote(log_out.at[h], log_in.at[h], log_s.at[0], log_r.at[h], {"sp": to})

    piece_dm = dm // 2
    pieces = 4

    def chain_copy(h, c, to):
        lines = pl.ds(c // 2 * piece_dm, piece_dm)
        cols = pl.ds(c % 2 * piece_dm, piece_dm)
        at = h * pieces + c
        return remote(
            state_out.at[h, lines, cols], state_in.at[h, lines, cols], chain_s.at[0], chain_r.at[at],
            {"sp": to},
        )

    def chain_logs(h):
        @pl.when(s == 0)
        def _():
            log_in[h] = jnp.full(log_in.shape[1:], floor_neg, f32)
            state_in[h] = jnp.zeros(state_in.shape[1:], bf16)

        @pl.when(s > 0)
        def _():
            log_copy(h, s - 1).wait_recv()

        total = totals[h : h + 1, 0:1]
        early = total + log_in[h, 0:1, 0:1]
        late = total + jnp.max(column(h), axis=0, keepdims=True)
        top = jnp.maximum(early, late)

        @pl.when(s < last)
        def _():
            log_out[h] = jnp.broadcast_to(top, log_out.shape[1:])
            log_copy(h, s + 1).start()

        factors[h, 0] = jnp.broadcast_to(jnp.exp(early - top), factors.shape[2:])
        factors[h, 1] = jnp.broadcast_to(jnp.exp(late - top), factors.shape[2:])

    def chain(h, low=0, high=pieces):
        if low == 0:
            chain_logs(h)
        early, late = factors[h, 0, 0:1, 0:1], factors[h, 1, 0:1, 0:1]
        for c in range(low, high):
            lines = pl.ds(c // 2 * piece_dm, piece_dm)
            cols = pl.ds(c % 2 * piece_dm, piece_dm)

            @pl.when(s > 0)
            def _():
                chain_copy(h, c, s - 1).wait_recv()

            @pl.when(s < last)
            def _():
                state_out[h, lines, cols] = (
                    early * state_in[h, lines, cols].astype(f32) + late * state_own[h, lines, cols]
                ).astype(bf16)
                chain_copy(h, c, s + 1).start()

    def chain_if(where, h, low=0, high=pieces):
        @pl.when(where)
        def _():
            chain(h, low, high)

    over(1, min(2, n_sp - 1), kv_forward)
    rest_weights(first)
    on_core(0, lambda: first_partials(first, 0))
    on_core(1, lambda: first_partials(first, 1))

    @pl.when(s > 0)
    def _():
        send_weights(fourth, fourth_own, splits + 2)

    own_partials(first)
    pass_weights(third, parity, splits + 1)
    over(1, min(2, n_sp - 1), own_span)
    partials(second)
    @pl.when(s == 0)
    def _():
        send_weights(fourth, fourth_own, splits + 2)

    def send_fourth():
        send_weights(fourth, fourth_all, splits + 3)

        @pl.when(s >= helper)
        def _():
            send_weights(fourth, fourth_rest, splits + 3)

    on_core(0, send_fourth)
    own_partials(second)
    @pl.when(s == helper)
    def _():
        query_copy().wait_recv()
        stick_first(1, False)

    over(1, min(2, n_sp - 1), far_span)

    @pl.when(s == helper)
    def _():
        pass_weights(fourth, fourth_own, splits + 2, 1)

    over(2, n_sp - 1, kv_forward)
    over(2, n_sp - 1, far_span)

    @pl.when(s == helper)
    def _():
        far_out[...] = stick_acc[1].astype(bf16)
        remote(far_out, far_in, far_s.at[0], far_r.at[0], {"sp": s + 1}).start()

    own_state(0)
    chain_if(s == 0, 0)
    on_core(1, send_fourth)

    @pl.when((s > 0) & (s != helper))
    def _():
        pass_weights(fourth, fourth_own, splits + 2, 1)

    chain_if(s == 1, 0)
    own_state(1)
    chain_if(s == 0, 1)
    partials(third)
    chain_if(s == 2, 0)
    own_partials(third)
    chain_if(s == 1, 1)

    @pl.when((s == 0) & (s != helper))
    def _():
        pass_weights(fourth, fourth_own, splits + 2, 1)

    partials(fourth)
    own_partials(fourth)
    loaded(gains, 10)
    chain_if((s == 2) & (t == 1), 1)
    over(2, n_sp - 1, own_span)
    chain_if((s == 2) & (t == 0), 1, 0, 2)
    width = heads * dm

    def mix_copy(at, low, high):
        return remote(
            mix.at[far_rows, pl.ds(low, high - low)], mix_in.at[:, pl.ds(low, high - low)],
            send_s.at[2], out_r.at[at], {"tp": other},
        )

    def stick_mix():
        for h in range(heads):
            cols = slice(h * ds, (h + 1) * ds)
            out = stick_acc[0, h]
            scale = lax.rsqrt(jnp.mean(out * out, axis=1, keepdims=True) + epsilon)
            mix[:, heads * dm + h * ds : heads * dm + (h + 1) * ds] = (
                out * scale * gains[:, heads * dm + h * ds : heads * dm + (h + 1) * ds]
            ).astype(bf16)
        mix_copy(heads, width, width + heads * ds).start()
        early_out[...] = dot(mix[my_rows, width:], wout[width:, :])

    @pl.when(s < last)
    def _():
        stick_mix()

    chain_if((s == 2) & (t == 0), 1, 2, pieces)

    causal = col_at <= row_at
    await_bytes(rb.at[QUERY], rs_r.at[QUERY])
    for h in range(heads):
        proj[QUERY, h] = finish(QUERY, h)
        masked = jnp.where(causal, u_rows[h : h + 1, :], floor_neg)
        top = jnp.max(masked, axis=1, keepdims=True)
        scores = dot(proj[QUERY, h], proj[KEY, h], ((1,), (1,))) * jnp.exp(masked - top)
        own_part[QUERY, h] = dot(scores.astype(bf16), proj[VALUE, h])
        tops[h] = jnp.broadcast_to(top, tops.shape[1:])


    @pl.when(s == last)
    def _():
        remote(far_out, far_in, far_s.at[0], far_r.at[0], {"sp": s - 1}).wait_recv()
        for h in range(heads):
            stick_acc[0, h] = stick_acc[0, h] + jnp.exp(stick_run[0, h]) * far_in[h].astype(f32)
        stick_mix()

    wout_copy.wait_recv()

    def mix_head(h, lines):
        carried_max = log_in[h, 0:1, 0:1]
        top = tops[h, lines, 0:1]
        running = jnp.maximum(carried_max, top)
        total = jnp.exp(top - running) * own_part[QUERY, h, lines] + jnp.exp(
            carried_max - running
        ) * dot(proj[QUERY, h, lines], state_in[h])
        gate = (own_part[GATE, h, lines] + rb[GATE, h, lines].astype(f32)).astype(bf16)
        gated = total / (1.0 + jnp.exp(-gate.astype(f32)))
        scale = lax.rsqrt(jnp.mean(gated * gated, axis=1, keepdims=True) + epsilon)
        cols = slice(h * dm, (h + 1) * dm)
        mix[lines, cols] = (gated * scale * gains[:, cols]).astype(bf16)

    for h in range(heads):
        chain_if(s > 2, h)
        if h == 0:
            mix_copy(heads, width, width + heads * ds).wait_recv()
            early_out[...] = early_out[...] + dot(mix_in[:, width:], wout_in[width:, :])
        await_bytes(rb.at[GATE, h], rs_r.at[GATE + h])
        mix_head(h, far_rows)
        mix_copy(h, h * dm, (h + 1) * dm).start()
        mix_head(h, my_rows)

    early_out[...] = early_out[...] + dot(mix[my_rows, :width], wout[:width, :])
    for h in range(heads):
        cols = slice(h * dm, (h + 1) * dm)
        mix_copy(h, h * dm, (h + 1) * dm).wait_recv()
        total = early_out[...] + dot(mix_in[:, cols], wout_in[cols, :])
        if h < heads - 1:
            early_out[...] = total
        else:
            out_ref[...] = total.astype(bf16)

    def sent_rows(where, count, sem):
        @pl.when(where)
        def _():
            sent_bytes(wout.at[pl.ds(0, count)], sem)

    quarter = block * width // (4 * features)
    moved = [8 * lines * block // features for lines in (cut, rows - cut)]
    for core in range(2):
        sent_rows((t == core) & (s < helper), moved[core] + 9 * quarter, send_s.at[0])
        sent_rows((t == core) & (s >= helper), moved[core] + 10 * quarter, send_s.at[0])
    sums = 4 * rows * width // features
    sent_rows(s == 0, sums, send_s.at[1])
    sent_rows((s > 0) & (s < helper), sums + 7 * quarter, send_s.at[1])
    sent_rows(s == helper, sums + 13 * quarter, send_s.at[1])
    sent_rows(s == last, sums + 6 * quarter, send_s.at[1])
    sent_bytes(wout.at[pl.ds(0, (rows * half_feat + half * wout.shape[0]) // features)], send_s.at[2])
    wout_copy.wait_send()

    @pl.when(s == helper)
    def _():
        remote(far_out, far_in, far_s.at[0], far_r.at[0], {"sp": s + 1}).wait_send()

    @pl.when(s == last)
    def _():
        query_copy().wait_send()

    @pl.when(s < last)
    def _():
        sent_bytes(log_out, log_s.at[0])
        sent_bytes(state_out, chain_s.at[0])

    def kv_done(d, c):
        @pl.when((s < helper) & (s >= d - 1))
        def _():
            kv_copy(d).wait_send()

        return c

    lax.fori_loop(1, n_sp - 1, kv_done, 0)


def per_device(
    n_sp,
    tokens,
    norm_gain,
    memory_query,
    memory_key,
    memory_value,
    memory_outgate,
    memory_ingate,
    memory_forget,
    forget_bias,
    forget_shift,
    stick_query,
    stick_key,
    stick_value,
    stick_bias,
    memory_gain,
    stick_gain,
    out_memory,
    out_stick,
):
    rows, half_feat = tokens.shape[1:]
    features = 2 * half_feat
    heads = forget_bias.shape[0]
    block, width = memory_query.shape
    dm = width // heads
    stick_width = stick_query.shape[1]
    ds = stick_width // heads
    lanes = 128
    half = rows // 2

    vmem = pl.BlockSpec(memory_space=pltpu.VMEM)
    anyw = pl.BlockSpec(memory_space=pl.ANY)
    dma = pltpu.SemaphoreType.DMA
    out = pl.pallas_call(
        functools.partial(kernel, n_sp),
        out_shape=pltpu.VMEM((half, features), bf16),
        in_specs=[anyw] * 18,
        out_specs=vmem,
        scratch_shapes=[
            pltpu.VMEM((rows, half_feat), bf16),
            pltpu.VMEM((1, features), f32),
            pltpu.VMEM((2, heads, features), bf16),
            pltpu.VMEM((heads, rows), f32),
            pltpu.VMEM((1, heads), f32),
            pltpu.VMEM((1, heads), f32),
            pltpu.VMEM((1, width + stick_width), f32),
            pltpu.VMEM((rows, half_feat), bf16),
            pltpu.VMEM((rows, features), bf16),
            pltpu.VMEM((2, 2, rows, block), bf16),
            pltpu.VMEM((4, block, width), bf16),
            pltpu.VMEM((4, heads, block, dm), bf16),
            pltpu.VMEM((3, features, stick_width), bf16),
            pltpu.VMEM((width + stick_width, features), bf16),
            pltpu.VMEM((4, heads, rows, dm), bf16),
            pltpu.VMEM((4, heads, rows, dm), bf16),
            pltpu.VMEM((4, heads, rows, dm), f32),
            pltpu.VMEM((4, heads, rows, dm), bf16),
            pltpu.VMEM((2, rows, stick_width), bf16),
            pltpu.VMEM((n_sp - 1, 2, rows, stick_width), bf16),
            pltpu.VMEM((2, heads, rows, ds), f32),
            pltpu.VMEM((2, heads, rows, ds), f32),
            pltpu.VMEM((heads, rows, ds), bf16),
            pltpu.VMEM((heads, rows, ds), bf16),
            pltpu.VMEM((16, features), bf16),
            pltpu.VMEM((lanes, rows), f32),
            pltpu.VMEM((rows, lanes), f32),
            pltpu.VMEM((8, lanes), f32),
            pltpu.VMEM((heads, rows, lanes), f32),
            pltpu.VMEM((heads, dm, dm), f32),
            pltpu.VMEM((heads, dm, dm), bf16),
            pltpu.VMEM((heads, dm, dm), bf16),
            pltpu.VMEM((heads, 8, lanes), f32),
            pltpu.VMEM((heads, 8, lanes), f32),
            pltpu.VMEM((heads, 2, 8, lanes), f32),
            pltpu.VMEM((rows, width + stick_width), bf16),
            pltpu.VMEM((half, width + stick_width), bf16),
            pltpu.VMEM((width + stick_width, features), bf16),
            pltpu.VMEM((half, features), f32),
            dma((11,)),
            dma((4,)),
            dma((2,)),
            dma((2,)),
            dma((1,)),
            dma((6,)),
            dma((4,)),
            dma((5,)),
            dma((n_sp - 2,)),
            dma((n_sp - 2,)),
            dma((1,)),
            dma((1,)),
            dma((1,)),
            dma((4 * heads,)),
            dma((1,)),
            dma((heads,)),
            dma((heads + 1,)),
        ],
        compiler_params=pltpu.CompilerParams(
            collective_id=0, has_side_effects=True, vmem_limit_bytes=60 * 1024 * 1024
        ),
    )(
        tokens[0],
        norm_gain[None],
        memory_ingate.T,
        memory_forget.T,
        forget_bias[None],
        forget_shift[0].T,
        stick_bias[None],
        memory_gain[None],
        stick_gain[None],
        memory_key,
        memory_value,
        memory_query,
        memory_outgate,
        stick_query,
        stick_key,
        stick_value,
        out_memory,
        out_stick,
    )
    return out[None]


def solution(mesh):
    assert mesh.shape["fs"] == 4 and mesh.shape["tp"] == 2
    return jax.shard_map(
        functools.partial(per_device, mesh.shape["sp"]),
        mesh=mesh,
        in_specs=(
            P("fs", "sp", "tp"),
            P(),
            P("fs", "tp"),
            P("fs", "tp"),
            P("fs", "tp"),
            P("fs", "tp"),
            P(None, "tp"),
            P(None, "tp"),
            P("tp"),
            P("fs", "sp", "tp"),
            P(None, "tp"),
            P(None, "tp"),
            P(None, "tp"),
            P("tp"),
            P("tp"),
            P("tp"),
            P("tp", None),
            P("tp", None),
        ),
        out_specs=P("fs", ("sp", "tp"), None),
        check_vma=False,
    )
```

```python
import functools

import jax
import jax.numpy as jnp
from jax import lax
from jax.experimental import pallas as pl
from jax.experimental.pallas import tpu as pltpu
from jax.sharding import PartitionSpec as P

MESH = pl.DeviceIdType.MESH
epsilon = 1e-06
floor_neg = -1e30
f32 = jnp.float32
bf16 = jnp.bfloat16

KEY, VALUE, QUERY, GATE = 0, 1, 2, 3


def dot(a, b, dims=((1,), (0,))):
    return lax.dot_general(a, b, (dims, ((), ())), preferred_element_type=f32)


def softplus(z):
    return jnp.maximum(z, 0.0) + jnp.log(1.0 + jnp.exp(-jnp.abs(z)))


def kernel(
    n_sp,
    tok_hbm,
    gain_hbm,
    ingate_hbm,
    forget_hbm,
    bias_hbm,
    shift_hbm,
    sbias_hbm,
    mgain_hbm,
    sgain_hbm,
    wk_hbm,
    wv_hbm,
    wq_hbm,
    wo_hbm,
    sq_hbm,
    sk_hbm,
    sv_hbm,
    om_hbm,
    os_hbm,
    out_ref,
    tok_ref,
    gain_ref,
    gate_in,
    shift_ref,
    bias_ref,
    sbias_ref,
    gains,
    tok_in,
    nrm,
    xg,
    wm,
    wg,
    ws,
    wout,
    sb,
    rb,
    own_part,
    proj,
    queries,
    kv,
    stick_acc,
    stick_run,
    far_out,
    far_in,
    gw,
    u_rows,
    u_cols,
    totals,
    tops,
    state_own,
    state_in,
    state_out,
    log_in,
    log_out,
    factors,
    mix,
    mix_in,
    wout_in,
    early_out,
    load_sem,
    send_s,
    tok_r,
    a2a_r,
    fwd_r,
    w_r,
    z_r,
    rs_r,
    kv_s,
    kv_r,
    far_s,
    far_r,
    chain_s,
    chain_r,
    log_s,
    log_r,
    out_r,
):
    f = lax.axis_index("fs")
    s = lax.axis_index("sp")
    t = lax.axis_index("tp")
    rows, half_feat = tok_ref.shape
    features = wout.shape[1]
    heads = state_own.shape[0]
    dm = state_own.shape[1]
    ds = stick_acc.shape[3]
    block = wm.shape[1]
    half = rows // 2
    other = 1 - t
    last = n_sp - 1
    helper = n_sp - 2

    def flip(bits):
        if bits == 1:
            return f + 1 - 2 * (f % 2)
        if bits == 2:
            return f + 2 - 4 * (f // 2)
        return 3 - f

    def remote(src, dst, send, recv, device):
        return pltpu.make_async_remote_copy(
            src_ref=src,
            dst_ref=dst,
            send_sem=send,
            recv_sem=recv,
            device_id=device,
            device_id_type=MESH,
        )

    barrier = pltpu.get_barrier_semaphore()
    pl.semaphore_signal(barrier, inc=1, device_id={"tp": other}, device_id_type=MESH)
    for bits in (1, 2):
        pl.semaphore_signal(barrier, inc=1, device_id={"fs": flip(bits)}, device_id_type=MESH)

    @pl.when(s > 0)
    def _():
        pl.semaphore_signal(barrier, inc=1, device_id={"sp": s - 1}, device_id_type=MESH)

    @pl.when(s < last)
    def _():
        pl.semaphore_signal(barrier, inc=1, device_id={"sp": s + 1}, device_id_type=MESH)

    def load(src, dst, at):
        return pltpu.make_async_copy(src, dst, load_sem.at[at])

    load(tok_hbm, tok_ref, 0).start()
    load(wk_hbm, wm.at[KEY], 1).start()
    load(wv_hbm, wm.at[VALUE], 1).start()
    load(gain_hbm, gain_ref, 2).start()
    load(sq_hbm, ws.at[0], 3).start()
    load(sk_hbm, ws.at[1], 3).start()
    load(sv_hbm, ws.at[2], 3).start()
    load(wq_hbm, wm.at[QUERY], 4).start()
    load(wo_hbm, wm.at[GATE], 4).start()
    load(ingate_hbm, gate_in.at[0], 5).start()
    load(forget_hbm, gate_in.at[1], 5).start()
    load(shift_hbm, shift_ref, 8).start()
    load(bias_hbm, bias_ref, 6).start()
    load(sbias_hbm, sbias_ref, 7).start()
    load(om_hbm, wout.at[pl.ds(0, heads * dm)], 9).start()
    load(os_hbm, wout.at[pl.ds(heads * dm, heads * ds)], 9).start()
    load(mgain_hbm, gains.at[:, pl.ds(0, heads * dm)], 10).start()
    load(sgain_hbm, gains.at[:, pl.ds(heads * dm, heads * ds)], 10).start()

    def loaded(ref, at):
        pltpu.make_async_copy(ref, ref, load_sem.at[at]).wait()

    peers = 3 + jnp.where(s > 0, 1, 0) + jnp.where(s < last, 1, 0)
    pl.semaphore_wait(barrier, peers)

    loaded(tok_ref, 0)
    tok_copy = remote(tok_ref, tok_in, send_s.at[2], tok_r.at[0], {"tp": other})

    def role(p, h):
        return (p + h) % 2

    def pair_bits(p, h):
        return 1 + role(p, h)

    def sum_bits(p, h):
        return 2 - role(p, h)

    first, second = [(KEY, 0), (VALUE, 0)], [(KEY, 1), (VALUE, 1)]
    third, fourth = [(QUERY, h) for h in range(heads)], [(GATE, h) for h in range(heads)]
    def part(number, count, parts=1, offset=0):
        size = block // count
        return pl.ds(pl.multiple_of(number * size, size) + offset * (size // parts), size // parts)

    parity, rest = part(s % 2, 2), part(1 - s % 2, 2)
    splits = 2
    fourth_own, fourth_rest, fourth_all = part(s % 2, 4), part(1 - s % 2, 4), part(1, 2)

    def stage(p, h):
        return h if p < 2 else p

    def weight_copy(p, h, lines, at):
        return remote(
            wm.at[p, lines, pl.ds(h * dm, dm)], wg.at[p, h, lines], send_s.at[0],
            w_r.at[at], {"fs": flip(pair_bits(p, h))},
        )

    def pass_copy(p, h, lines, at, to):
        return remote(
            wg.at[p, h, lines], wg.at[p, h, lines], send_s.at[1], z_r.at[stage(p, h)], {"sp": to}
        )

    def both(p, h, lines):
        return wg.at[pl.ds(0, 2), h, lines] if p < 2 else wg.at[p, :, lines]

    def await_bytes(ref, sem):
        remote(ref, ref, send_s.at[0], sem, {"tp": other}).wait_recv()

    def sent_bytes(ref, sem):
        remote(ref, ref, sem, z_r.at[0], {"tp": other}).wait_send()

    def send_weights(items, lines, at):
        for p, h in items:
            weight_copy(p, h, lines, at).start()

    def pass_weights(items, lines, at, sem=0):
        p, h = items[0]
        await_bytes(both(p, h, lines), w_r.at[at])
        down = (s > 0) & (s < last) if items is fourth else s > 0
        for p, h in items:
            @pl.when(down)
            def _():
                pass_copy(p, h, lines, sem, s - 1).start()

            if items is fourth:
                continue

            @pl.when(s == helper)
            def _():
                pass_copy(p, h, lines, 2 + sem, s + 1).start()

    def first_lines(c):
        return part(s % 2, 2, splits, c)

    def rest_weights(items):
        p, h = items[0]
        if items is not fourth:
            await_bytes(both(p, h, rest), z_r.at[stage(p, h)])
            return

        @pl.when(s < helper)
        def _():
            await_bytes(both(p, h, fourth_all), w_r.at[splits + 3])
            await_bytes(both(p, h, fourth_rest), z_r.at[stage(p, h)])

        @pl.when(s >= helper)
        def _():
            await_bytes(both(p, h, pl.ds(0, block - block // 4)), w_r.at[splits + 3])

    def on_core(where, step):
        @pl.when(t == where)
        def _():
            step()

    on_core(1, tok_copy.start)
    loaded(wm.at[pl.ds(KEY, 2)], 1)
    for c in range(splits):
        send_weights(first, first_lines(c), c)
    send_weights(second, parity, splits)
    on_core(0, tok_copy.start)
    tok_copy.wait_recv()
    loaded(gain_ref, 2)

    step_rows = 32
    own_cols = pl.ds(pl.multiple_of(t * half_feat, half_feat), half_feat)
    far_cols = pl.ds(pl.multiple_of(other * half_feat, half_feat), half_feat)

    def norm_rows(i, _):
        at = pl.ds(pl.multiple_of(i * step_rows, step_rows), step_rows)
        own = tok_ref[at, :].astype(f32)
        far = tok_in[at, :].astype(f32)
        total = jnp.sum(own * own, axis=1, keepdims=True) + jnp.sum(far * far, axis=1, keepdims=True)
        scale = lax.rsqrt(total / (2 * half_feat) + epsilon)
        nrm[at, own_cols] = (own * scale * gain_ref[:, own_cols]).astype(bf16)
        nrm[at, far_cols] = (far * scale * gain_ref[:, far_cols]).astype(bf16)
        return 0

    lax.fori_loop(0, rows // step_rows, norm_rows, 0)

    my_rows = pl.ds(pl.multiple_of(t * half, half), half)
    cut = rows * 7 // 16
    core_rows = (pl.ds(0, cut), pl.ds(cut, rows - cut))

    def feature_block(index):
        return pl.ds(pl.multiple_of(index * block, block), block)

    def a2a_copy(core, r, which):
        lines = core_rows[core]
        to = flip(2 - r)
        return remote(
            nrm.at[lines, feature_block(to if which == 0 else flip(3))],
            xg.at[r, which, lines],
            send_s.at[0],
            a2a_r.at[which],
            {"fs": to},
        )

    def fwd_copy(core, r, which):
        lines = core_rows[core]
        return remote(
            xg.at[r, which, lines], xg.at[r, which, lines], send_s.at[0], fwd_r.at[0], {"tp": other}
        )

    def a2a_start(core):
        for r in range(2):
            for which in range(2):
                a2a_copy(core, r, which).start()

    on_core(0, lambda: a2a_start(0))
    on_core(1, lambda: a2a_start(1))
    loaded(wm.at[pl.ds(QUERY, 2)], 4)
    send_weights(third, parity, splits + 1)
    loaded(ws, 3)
    normed = nrm[...]
    queries[0] = dot(normed, ws[0]).astype(bf16)

    def query_copy():
        return remote(queries.at[0], queries.at[1], far_s.at[0], far_r.at[0], {"sp": s - 1})

    def kv_copy(d):
        return remote(kv.at[d - 1], kv.at[d], kv_s.at[d - 1], kv_r.at[d - 1], {"sp": s + 1})

    def kv_send(d):
        @pl.when((s < helper) & (s >= d - 1))
        def _():
            kv_copy(d).start()

    def kv_project():
        normed = nrm[...]
        kv[0, 0] = dot(normed, ws[1]).astype(bf16)
        kv[0, 1] = dot(normed, ws[2]).astype(bf16)
        kv_send(1)

    def pass_first():
        for c in range(splits):
            pass_weights(first, first_lines(c), c)

    on_core(0, kv_project)
    pass_first()
    on_core(1, kv_project)

    row_at = lax.broadcasted_iota(jnp.int32, (rows, rows), 0)
    col_at = lax.broadcasted_iota(jnp.int32, (rows, rows), 1)
    loaded(gate_in, 5)
    loaded(shift_ref, 8)
    load(bias_hbm, bias_ref, 6).wait()
    load(sbias_hbm, sbias_ref, 7).wait()
    gw[...] = jnp.zeros(gw.shape, bf16)
    gw[0:heads, :] = gate_in[0]
    gw[8 : 8 + heads, :] = gate_in[1]
    gate = dot(gw[...], normed, ((1,), (1,)))
    triu = (row_at <= col_at).astype(f32)
    u_rows[...] = jnp.zeros(u_rows.shape, f32)
    for h in range(heads):
        log_forget = shift_ref[h : h + 1, :] - softplus(-(gate[8 + h : 9 + h, :] + bias_ref[0:1, h : h + 1]))
        cumulative = lax.dot_general(
            jnp.broadcast_to(log_forget, (8, rows)), triu, (((1,), (0,)), ((), ())),
            precision=lax.Precision.HIGHEST, preferred_element_type=f32,
        )
        u_rows[h : h + 1, :] = gate[h : h + 1, :] - cumulative[0:1, :]
        totals[h : h + 1, :] = jnp.broadcast_to(
            cumulative[0:1, rows - 1 : rows], (1, totals.shape[1])
        )
    u_cols[...] = jnp.transpose(u_rows[...])

    pass_weights(second, parity, splits)

    @pl.when(s == last)
    def _():
        query_copy().start()


    def stick_part(at, h, kv_at, diagonal):
        cols = slice(h * ds, (h + 1) * ds)
        z = dot(queries[at, :, cols], kv[kv_at, 0, :, cols], ((1,), (1,)))
        z = z * ds ** (-0.5) + sbias_ref[0:1, h : h + 1]
        keep = -softplus(z)
        visible = col_at < row_at
        if diagonal:
            kept = jnp.where(visible, keep, 0.0)
        else:
            kept = keep
        strict = (row_at > col_at).astype(bf16)
        high = kept.astype(bf16)
        low = (kept - high.astype(f32)).astype(bf16)
        after = dot(high, strict) + dot(low, strict)
        weights = jnp.exp(z + keep + after)
        if diagonal:
            weights = jnp.where(visible, weights, 0.0)
        part = dot(weights.astype(bf16), kv[kv_at, 1, :, cols])
        return part, after[:, 0:1] + kept[:, 0:1]

    def stick_first(at, diagonal):
        for h in range(heads):
            part, keep = stick_part(at, h, 0, diagonal)
            stick_acc[at, h] = part
            stick_run[at, h] = jnp.broadcast_to(keep, stick_run.shape[2:])

    def kv_forward(d):
        @pl.when((s >= d) & (s <= helper))
        def _():
            remote(kv.at[d - 1], kv.at[d], kv_s.at[d - 1], kv_r.at[d - 1], {"sp": s - 1}).wait_recv()

        @pl.when((s >= d) & (s < helper))
        def _():
            kv_copy(d + 1).start()

    def stick_span(at, d):
        for h in range(heads):
            part, keep = stick_part(at, h, d, False)
            stick_acc[at, h] = stick_acc[at, h] + jnp.exp(stick_run[at, h]) * part
            stick_run[at, h] = stick_run[at, h] + keep

    def own_span(d):
        @pl.when((s >= d) & (s <= helper))
        def _():
            stick_span(0, d)

    def far_span(d):
        @pl.when(s == helper)
        def _():
            stick_span(1, d)

    def over(low, high, step):
        if high > low:
            lax.fori_loop(low, high, lambda d, c: (step(d), c)[1], 0)

    loaded(wout, 9)
    wout_copy = remote(wout, wout_in, send_s.at[3], tok_r.at[1], {"tp": other})
    wout_copy.start()
    stick_first(0, True)

    def a2a_forward(core):
        for which in range(2):
            await_bytes(xg.at[:, which, core_rows[core]], a2a_r.at[which])
            for r in range(2):
                fwd_copy(core, r, which).start()

    on_core(0, lambda: a2a_forward(0))
    on_core(1, lambda: a2a_forward(1))
    far_rows = pl.ds(pl.multiple_of(other * half, half), half)

    def rs_sem(p, h):
        return h if p < 2 else p + (h if p == GATE else 0)

    def rs_copy(p, h, lines):
        return remote(
            sb.at[p, h, lines], rb.at[p, h, lines], send_s.at[1], rs_r.at[rs_sem(p, h)],
            {"fs": flip(sum_bits(p, h))},
        )

    def partials(items):
        rest_weights(items)
        for p, h in items:
            cols = slice(h * dm, (h + 1) * dm)
            r = role(p, h)
            sb[p, h] = (dot(xg[r, 0], wm[p, :, cols]) + dot(xg[r, 1], wg[p, h])).astype(bf16)
            rs_copy(p, h, pl.ds(0, rows)).start()

    def first_partials(items, core):
        for at in (core, 1 - core):
            lines = core_rows[at]
            if at != core:
                await_bytes(xg.at[:, :, lines], fwd_r.at[0])
            for p, h in items:
                cols = slice(h * dm, (h + 1) * dm)
                r = role(p, h)
                sb[p, h, lines] = (
                    dot(xg[r, 0, lines], wm[p, :, cols]) + dot(xg[r, 1, lines], wg[p, h])
                ).astype(bf16)
                rs_copy(p, h, lines).start()

    def own_partials(items):
        for p, h in items:
            cols = slice(h * dm, (h + 1) * dm)
            own_part[p, h] = dot(nrm[:, feature_block(f)], wm[p, :, cols]) + dot(
                nrm[:, feature_block(flip(pair_bits(p, h)))], wg[p, h]
            )

    def finish(p, h):
        return (own_part[p, h] + rb[p, h].astype(f32)).astype(bf16)

    def column(h):
        return u_cols[:, h : h + 1]

    def own_state(h):
        await_bytes(rb.at[pl.ds(0, 2), h], rs_r.at[h])
        proj[KEY, h] = (finish(KEY, h).astype(f32) * dm ** (-0.5)).astype(bf16)
        proj[VALUE, h] = finish(VALUE, h)
        u = column(h)
        top = jnp.max(u, axis=0, keepdims=True)
        weighted = (proj[KEY, h].astype(f32) * jnp.exp(u - top)).astype(bf16)
        state_own[h] = dot(weighted, proj[VALUE, h], ((0,), (0,)))

    def log_copy(h, to):
        return remote(log_out.at[h], log_in.at[h], log_s.at[0], log_r.at[h], {"sp": to})

    piece_dm = dm // 2
    pieces = 4

    def chain_copy(h, c, to):
        lines = pl.ds(c // 2 * piece_dm, piece_dm)
        cols = pl.ds(c % 2 * piece_dm, piece_dm)
        at = h * pieces + c
        return remote(
            state_out.at[h, lines, cols], state_in.at[h, lines, cols], chain_s.at[0], chain_r.at[at],
            {"sp": to},
        )

    def chain_logs(h):
        @pl.when(s == 0)
        def _():
            log_in[h] = jnp.full(log_in.shape[1:], floor_neg, f32)
            state_in[h] = jnp.zeros(state_in.shape[1:], bf16)

        @pl.when(s > 0)
        def _():
            log_copy(h, s - 1).wait_recv()

        total = totals[h : h + 1, 0:1]
        early = total + log_in[h, 0:1, 0:1]
        late = total + jnp.max(column(h), axis=0, keepdims=True)
        top = jnp.maximum(early, late)

        @pl.when(s < last)
        def _():
            log_out[h] = jnp.broadcast_to(top, log_out.shape[1:])
            log_copy(h, s + 1).start()

        factors[h, 0] = jnp.broadcast_to(jnp.exp(early - top), factors.shape[2:])
        factors[h, 1] = jnp.broadcast_to(jnp.exp(late - top), factors.shape[2:])

    def chain(h, low=0, high=pieces):
        if low == 0:
            chain_logs(h)
        early, late = factors[h, 0, 0:1, 0:1], factors[h, 1, 0:1, 0:1]
        for c in range(low, high):
            lines = pl.ds(c // 2 * piece_dm, piece_dm)
            cols = pl.ds(c % 2 * piece_dm, piece_dm)

            @pl.when(s > 0)
            def _():
                chain_copy(h, c, s - 1).wait_recv()

            @pl.when(s < last)
            def _():
                state_out[h, lines, cols] = (
                    early * state_in[h, lines, cols].astype(f32) + late * state_own[h, lines, cols]
                ).astype(bf16)
                chain_copy(h, c, s + 1).start()

    def chain_if(where, h, low=0, high=pieces):
        @pl.when(where)
        def _():
            chain(h, low, high)

    over(1, min(2, n_sp - 1), kv_forward)
    rest_weights(first)
    on_core(0, lambda: first_partials(first, 0))
    on_core(1, lambda: first_partials(first, 1))
    send_weights(fourth, fourth_own, splits + 2)
    own_partials(first)
    pass_weights(third, parity, splits + 1)
    over(1, min(2, n_sp - 1), own_span)
    partials(second)
    def send_fourth():
        send_weights(fourth, fourth_all, splits + 3)

        @pl.when(s >= helper)
        def _():
            send_weights(fourth, fourth_rest, splits + 3)

    send_fourth()
    own_partials(second)
    @pl.when(s == helper)
    def _():
        query_copy().wait_recv()
        stick_first(1, False)

    over(1, min(2, n_sp - 1), far_span)

    @pl.when(s == helper)
    def _():
        pass_weights(fourth, fourth_own, splits + 2, 1)

    over(2, n_sp - 1, kv_forward)
    over(2, n_sp - 1, far_span)

    @pl.when(s == helper)
    def _():
        far_out[...] = stick_acc[1].astype(bf16)
        remote(far_out, far_in, far_s.at[0], far_r.at[0], {"sp": s + 1}).start()

    own_state(0)
    chain_if(s == 0, 0)

    @pl.when((s > 0) & (s < helper) & (t == 0))
    def _():
        pass_weights(fourth, fourth_own, splits + 2, 1)

    chain_if(s == 1, 0)
    own_state(1)
    chain_if(s == 0, 1)
    @pl.when((s > 0) & (s < helper) & (t == 1))
    def _():
        pass_weights(fourth, fourth_own, splits + 2, 1)

    partials(third)
    chain_if(s == 2, 0)
    own_partials(third)
    chain_if(s == 1, 1)

    @pl.when((s == 0) | (s == last))
    def _():
        await_bytes(both(GATE, 0, fourth_own), w_r.at[splits + 2])

    partials(fourth)
    own_partials(fourth)
    loaded(gains, 10)
    chain_if((s == 2) & (t == 1), 1)
    over(2, n_sp - 1, own_span)
    chain_if((s == 2) & (t == 0), 1, 0, 2)
    width = heads * dm

    def mix_copy(at, low, high):
        return remote(
            mix.at[far_rows, pl.ds(low, high - low)], mix_in.at[:, pl.ds(low, high - low)],
            send_s.at[2], out_r.at[at], {"tp": other},
        )

    def stick_mix():
        for h in range(heads):
            cols = slice(h * ds, (h + 1) * ds)
            out = stick_acc[0, h]
            scale = lax.rsqrt(jnp.mean(out * out, axis=1, keepdims=True) + epsilon)
            mix[:, heads * dm + h * ds : heads * dm + (h + 1) * ds] = (
                out * scale * gains[:, heads * dm + h * ds : heads * dm + (h + 1) * ds]
            ).astype(bf16)
        mix_copy(heads, width, width + heads * ds).start()
        early_out[...] = dot(mix[my_rows, width:], wout[width:, :])

    @pl.when(s < last)
    def _():
        stick_mix()

    chain_if((s == 2) & (t == 0), 1, 2, pieces)

    causal = col_at <= row_at
    await_bytes(rb.at[QUERY], rs_r.at[QUERY])
    for h in range(heads):
        proj[QUERY, h] = finish(QUERY, h)
        masked = jnp.where(causal, u_rows[h : h + 1, :], floor_neg)
        top = jnp.max(masked, axis=1, keepdims=True)
        scores = dot(proj[QUERY, h], proj[KEY, h], ((1,), (1,))) * jnp.exp(masked - top)
        own_part[QUERY, h] = dot(scores.astype(bf16), proj[VALUE, h])
        tops[h] = jnp.broadcast_to(top, tops.shape[1:])


    @pl.when(s == last)
    def _():
        remote(far_out, far_in, far_s.at[0], far_r.at[0], {"sp": s - 1}).wait_recv()
        for h in range(heads):
            stick_acc[0, h] = stick_acc[0, h] + jnp.exp(stick_run[0, h]) * far_in[h].astype(f32)
        stick_mix()

    wout_copy.wait_recv()

    def mix_head(h, lines):
        carried_max = log_in[h, 0:1, 0:1]
        top = tops[h, lines, 0:1]
        running = jnp.maximum(carried_max, top)
        total = jnp.exp(top - running) * own_part[QUERY, h, lines] + jnp.exp(
            carried_max - running
        ) * dot(proj[QUERY, h, lines], state_in[h])
        gate = (own_part[GATE, h, lines] + rb[GATE, h, lines].astype(f32)).astype(bf16)
        gated = total / (1.0 + jnp.exp(-gate.astype(f32)))
        scale = lax.rsqrt(jnp.mean(gated * gated, axis=1, keepdims=True) + epsilon)
        cols = slice(h * dm, (h + 1) * dm)
        mix[lines, cols] = (gated * scale * gains[:, cols]).astype(bf16)

    for h in range(heads):
        chain_if(s > 2, h)
        if h == 0:
            mix_copy(heads, width, width + heads * ds).wait_recv()
            early_out[...] = early_out[...] + dot(mix_in[:, width:], wout_in[width:, :])
        await_bytes(rb.at[GATE, h], rs_r.at[GATE + h])
        mix_head(h, far_rows)
        mix_copy(h, h * dm, (h + 1) * dm).start()
        mix_head(h, my_rows)

    early_out[...] = early_out[...] + dot(mix[my_rows, :width], wout[:width, :])
    for h in range(heads):
        cols = slice(h * dm, (h + 1) * dm)
        mix_copy(h, h * dm, (h + 1) * dm).wait_recv()
        total = early_out[...] + dot(mix_in[:, cols], wout_in[cols, :])
        if h < heads - 1:
            early_out[...] = total
        else:
            out_ref[...] = total.astype(bf16)

    def sent_rows(where, count, sem):
        @pl.when(where)
        def _():
            sent_bytes(wout.at[pl.ds(0, count)], sem)

    quarter = block * width // (4 * features)
    moved = [8 * lines * block // features for lines in (cut, rows - cut)]
    for core in range(2):
        sent_rows((t == core) & (s < helper), moved[core] + 9 * quarter, send_s.at[0])
        sent_rows((t == core) & (s >= helper), moved[core] + 10 * quarter, send_s.at[0])
    sums = 4 * rows * width // features
    sent_rows(s == 0, sums, send_s.at[1])
    sent_rows((s > 0) & (s < helper), sums + 7 * quarter, send_s.at[1])
    sent_rows(s == helper, sums + 13 * quarter, send_s.at[1])
    sent_rows(s == last, sums + 6 * quarter, send_s.at[1])
    sent_bytes(wout.at[pl.ds(0, (rows * half_feat + half * wout.shape[0]) // features)], send_s.at[2])
    wout_copy.wait_send()

    @pl.when(s == helper)
    def _():
        remote(far_out, far_in, far_s.at[0], far_r.at[0], {"sp": s + 1}).wait_send()

    @pl.when(s == last)
    def _():
        query_copy().wait_send()

    @pl.when(s < last)
    def _():
        sent_bytes(log_out, log_s.at[0])
        sent_bytes(state_out, chain_s.at[0])

    def kv_done(d, c):
        @pl.when((s < helper) & (s >= d - 1))
        def _():
            kv_copy(d).wait_send()

        return c

    lax.fori_loop(1, n_sp - 1, kv_done, 0)


def per_device(
    n_sp,
    tokens,
    norm_gain,
    memory_query,
    memory_key,
    memory_value,
    memory_outgate,
    memory_ingate,
    memory_forget,
    forget_bias,
    forget_shift,
    stick_query,
    stick_key,
    stick_value,
    stick_bias,
    memory_gain,
    stick_gain,
    out_memory,
    out_stick,
):
    rows, half_feat = tokens.shape[1:]
    features = 2 * half_feat
    heads = forget_bias.shape[0]
    block, width = memory_query.shape
    dm = width // heads
    stick_width = stick_query.shape[1]
    ds = stick_width // heads
    lanes = 128
    half = rows // 2

    vmem = pl.BlockSpec(memory_space=pltpu.VMEM)
    anyw = pl.BlockSpec(memory_space=pl.ANY)
    dma = pltpu.SemaphoreType.DMA
    out = pl.pallas_call(
        functools.partial(kernel, n_sp),
        out_shape=pltpu.VMEM((half, features), bf16),
        in_specs=[anyw] * 18,
        out_specs=vmem,
        scratch_shapes=[
            pltpu.VMEM((rows, half_feat), bf16),
            pltpu.VMEM((1, features), f32),
            pltpu.VMEM((2, heads, features), bf16),
            pltpu.VMEM((heads, rows), f32),
            pltpu.VMEM((1, heads), f32),
            pltpu.VMEM((1, heads), f32),
            pltpu.VMEM((1, width + stick_width), f32),
            pltpu.VMEM((rows, half_feat), bf16),
            pltpu.VMEM((rows, features), bf16),
            pltpu.VMEM((2, 2, rows, block), bf16),
            pltpu.VMEM((4, block, width), bf16),
            pltpu.VMEM((4, heads, block, dm), bf16),
            pltpu.VMEM((3, features, stick_width), bf16),
            pltpu.VMEM((width + stick_width, features), bf16),
            pltpu.VMEM((4, heads, rows, dm), bf16),
            pltpu.VMEM((4, heads, rows, dm), bf16),
            pltpu.VMEM((4, heads, rows, dm), f32),
            pltpu.VMEM((4, heads, rows, dm), bf16),
            pltpu.VMEM((2, rows, stick_width), bf16),
            pltpu.VMEM((n_sp - 1, 2, rows, stick_width), bf16),
            pltpu.VMEM((2, heads, rows, ds), f32),
            pltpu.VMEM((2, heads, rows, ds), f32),
            pltpu.VMEM((heads, rows, ds), bf16),
            pltpu.VMEM((heads, rows, ds), bf16),
            pltpu.VMEM((16, features), bf16),
            pltpu.VMEM((lanes, rows), f32),
            pltpu.VMEM((rows, lanes), f32),
            pltpu.VMEM((8, lanes), f32),
            pltpu.VMEM((heads, rows, lanes), f32),
            pltpu.VMEM((heads, dm, dm), f32),
            pltpu.VMEM((heads, dm, dm), bf16),
            pltpu.VMEM((heads, dm, dm), bf16),
            pltpu.VMEM((heads, 8, lanes), f32),
            pltpu.VMEM((heads, 8, lanes), f32),
            pltpu.VMEM((heads, 2, 8, lanes), f32),
            pltpu.VMEM((rows, width + stick_width), bf16),
            pltpu.VMEM((half, width + stick_width), bf16),
            pltpu.VMEM((width + stick_width, features), bf16),
            pltpu.VMEM((half, features), f32),
            dma((11,)),
            dma((4,)),
            dma((2,)),
            dma((2,)),
            dma((1,)),
            dma((6,)),
            dma((4,)),
            dma((5,)),
            dma((n_sp - 2,)),
            dma((n_sp - 2,)),
            dma((1,)),
            dma((1,)),
            dma((1,)),
            dma((4 * heads,)),
            dma((1,)),
            dma((heads,)),
            dma((heads + 1,)),
        ],
        compiler_params=pltpu.CompilerParams(
            collective_id=0, has_side_effects=True, vmem_limit_bytes=60 * 1024 * 1024
        ),
    )(
        tokens[0],
        norm_gain[None],
        memory_ingate.T,
        memory_forget.T,
        forget_bias[None],
        forget_shift[0].T,
        stick_bias[None],
        memory_gain[None],
        stick_gain[None],
        memory_key,
        memory_value,
        memory_query,
        memory_outgate,
        stick_query,
        stick_key,
        stick_value,
        out_memory,
        out_stick,
    )
    return out[None]


def solution(mesh):
    assert mesh.shape["fs"] == 4 and mesh.shape["tp"] == 2
    return jax.shard_map(
        functools.partial(per_device, mesh.shape["sp"]),
        mesh=mesh,
        in_specs=(
            P("fs", "sp", "tp"),
            P(),
            P("fs", "tp"),
            P("fs", "tp"),
            P("fs", "tp"),
            P("fs", "tp"),
            P(None, "tp"),
            P(None, "tp"),
            P("tp"),
            P("fs", "sp", "tp"),
            P(None, "tp"),
            P(None, "tp"),
            P(None, "tp"),
            P("tp"),
            P("tp"),
            P("tp"),
            P("tp", None),
            P("tp", None),
        ),
        out_specs=P("fs", ("sp", "tp"), None),
        check_vma=False,
    )
```

```python
import functools

import jax
import jax.numpy as jnp
from jax import lax
from jax.experimental import pallas as pl
from jax.experimental.pallas import tpu as pltpu
from jax.sharding import PartitionSpec as P

MESH = pl.DeviceIdType.MESH
epsilon = 1e-06
floor_neg = -1e30
f32 = jnp.float32
bf16 = jnp.bfloat16

KEY, VALUE, QUERY, GATE = 0, 1, 2, 3


def dot(a, b, dims=((1,), (0,))):
    return lax.dot_general(a, b, (dims, ((), ())), preferred_element_type=f32)


def softplus(z):
    return jnp.maximum(z, 0.0) + jnp.log(1.0 + jnp.exp(-jnp.abs(z)))


def kernel(
    n_sp,
    tok_hbm,
    gain_hbm,
    ingate_hbm,
    forget_hbm,
    bias_hbm,
    shift_hbm,
    sbias_hbm,
    mgain_hbm,
    sgain_hbm,
    wk_hbm,
    wv_hbm,
    wq_hbm,
    wo_hbm,
    sq_hbm,
    sk_hbm,
    sv_hbm,
    om_hbm,
    os_hbm,
    out_ref,
    tok_ref,
    gain_ref,
    gate_in,
    shift_ref,
    bias_ref,
    sbias_ref,
    gains,
    tok_in,
    nrm,
    xg,
    wm,
    wg,
    ws,
    wout,
    sb,
    rb,
    own_part,
    proj,
    queries,
    kv,
    stick_acc,
    stick_run,
    far_out,
    far_in,
    gw,
    u_rows,
    u_cols,
    totals,
    tops,
    state_own,
    state_in,
    state_out,
    log_in,
    log_out,
    factors,
    mix,
    mix_in,
    wout_in,
    early_out,
    load_sem,
    send_s,
    tok_r,
    a2a_r,
    fwd_r,
    w_r,
    z_r,
    rs_r,
    kv_s,
    kv_r,
    far_s,
    far_r,
    chain_s,
    chain_r,
    log_s,
    log_r,
    out_r,
):
    f = lax.axis_index("fs")
    s = lax.axis_index("sp")
    t = lax.axis_index("tp")
    rows, half_feat = tok_ref.shape
    features = wout.shape[1]
    heads = state_own.shape[0]
    dm = state_own.shape[1]
    ds = stick_acc.shape[3]
    block = wm.shape[1]
    half = rows // 2
    other = 1 - t
    last = n_sp - 1
    helper = n_sp - 2

    def flip(bits):
        if bits == 1:
            return f + 1 - 2 * (f % 2)
        if bits == 2:
            return f + 2 - 4 * (f // 2)
        return 3 - f

    def remote(src, dst, send, recv, device):
        return pltpu.make_async_remote_copy(
            src_ref=src,
            dst_ref=dst,
            send_sem=send,
            recv_sem=recv,
            device_id=device,
            device_id_type=MESH,
        )

    barrier = pltpu.get_barrier_semaphore()
    pl.semaphore_signal(barrier, inc=1, device_id={"tp": other}, device_id_type=MESH)
    for bits in (1, 2):
        pl.semaphore_signal(barrier, inc=1, device_id={"fs": flip(bits)}, device_id_type=MESH)

    @pl.when(s > 0)
    def _():
        pl.semaphore_signal(barrier, inc=1, device_id={"sp": s - 1}, device_id_type=MESH)

    @pl.when(s < last)
    def _():
        pl.semaphore_signal(barrier, inc=1, device_id={"sp": s + 1}, device_id_type=MESH)

    def load(src, dst, at):
        return pltpu.make_async_copy(src, dst, load_sem.at[at])

    load(tok_hbm, tok_ref, 0).start()
    load(wk_hbm, wm.at[KEY], 1).start()
    load(wv_hbm, wm.at[VALUE], 1).start()
    load(gain_hbm, gain_ref, 2).start()
    load(sq_hbm, ws.at[0], 3).start()
    load(sk_hbm, ws.at[1], 3).start()
    load(sv_hbm, ws.at[2], 3).start()
    load(wq_hbm, wm.at[QUERY], 4).start()
    load(wo_hbm, wm.at[GATE], 4).start()
    load(ingate_hbm, gate_in.at[0], 5).start()
    load(forget_hbm, gate_in.at[1], 5).start()
    load(shift_hbm, shift_ref, 8).start()
    load(bias_hbm, bias_ref, 6).start()
    load(sbias_hbm, sbias_ref, 7).start()
    load(om_hbm, wout.at[pl.ds(0, heads * dm)], 9).start()
    load(os_hbm, wout.at[pl.ds(heads * dm, heads * ds)], 9).start()
    load(mgain_hbm, gains.at[:, pl.ds(0, heads * dm)], 10).start()
    load(sgain_hbm, gains.at[:, pl.ds(heads * dm, heads * ds)], 10).start()

    def loaded(ref, at):
        pltpu.make_async_copy(ref, ref, load_sem.at[at]).wait()

    peers = 3 + jnp.where(s > 0, 1, 0) + jnp.where(s < last, 1, 0)
    pl.semaphore_wait(barrier, peers)

    loaded(tok_ref, 0)
    tok_copy = remote(tok_ref, tok_in, send_s.at[2], tok_r.at[0], {"tp": other})

    def role(p, h):
        return (p + h) % 2

    def pair_bits(p, h):
        return 1 + role(p, h)

    def sum_bits(p, h):
        return 2 - role(p, h)

    first, second = [(KEY, 0), (VALUE, 0)], [(KEY, 1), (VALUE, 1)]
    third, fourth = [(QUERY, h) for h in range(heads)], [(GATE, h) for h in range(heads)]
    def part(number, count, parts=1, offset=0):
        size = block // count
        return pl.ds(pl.multiple_of(number * size, size) + offset * (size // parts), size // parts)

    parity, rest = part(s % 2, 2), part(1 - s % 2, 2)
    splits = 2
    fourth_own, fourth_rest, fourth_all = part(s % 2, 4), part(1 - s % 2, 4), part(1, 2)

    def stage(p, h):
        return h if p < 2 else p

    def weight_copy(p, h, lines, at):
        return remote(
            wm.at[p, lines, pl.ds(h * dm, dm)], wg.at[p, h, lines], send_s.at[0],
            w_r.at[at], {"fs": flip(pair_bits(p, h))},
        )

    def pass_copy(p, h, lines, at, to):
        return remote(
            wg.at[p, h, lines], wg.at[p, h, lines], send_s.at[1], z_r.at[stage(p, h)], {"sp": to}
        )

    def both(p, h, lines):
        return wg.at[pl.ds(0, 2), h, lines] if p < 2 else wg.at[p, :, lines]

    def await_bytes(ref, sem):
        remote(ref, ref, send_s.at[0], sem, {"tp": other}).wait_recv()

    def sent_bytes(ref, sem):
        remote(ref, ref, sem, z_r.at[0], {"tp": other}).wait_send()

    def send_weights(items, lines, at):
        for p, h in items:
            weight_copy(p, h, lines, at).start()

    def pass_weights(items, lines, at, sem=0):
        p, h = items[0]
        await_bytes(both(p, h, lines), w_r.at[at])
        down = (s > 0) & (s < last) if items is fourth else s > 0
        for p, h in items:
            @pl.when(down)
            def _():
                pass_copy(p, h, lines, sem, s - 1).start()

            if items is fourth:
                continue

            @pl.when(s == helper)
            def _():
                pass_copy(p, h, lines, 2 + sem, s + 1).start()

    def first_lines(c):
        return part(s % 2, 2, splits, c)

    def rest_weights(items):
        p, h = items[0]
        if items is not fourth:
            await_bytes(both(p, h, rest), z_r.at[stage(p, h)])
            return

        @pl.when(s < helper)
        def _():
            await_bytes(both(p, h, fourth_all), w_r.at[splits + 3])
            await_bytes(both(p, h, fourth_rest), z_r.at[stage(p, h)])

        @pl.when(s >= helper)
        def _():
            await_bytes(both(p, h, pl.ds(0, block - block // 4)), w_r.at[splits + 3])

    def on_core(where, step):
        @pl.when(t == where)
        def _():
            step()

    on_core(1, tok_copy.start)
    loaded(wm.at[pl.ds(KEY, 2)], 1)
    for c in range(splits):
        send_weights(first, first_lines(c), c)
    send_weights(second, parity, splits)
    on_core(0, tok_copy.start)
    tok_copy.wait_recv()
    loaded(gain_ref, 2)

    step_rows = 32
    own_cols = pl.ds(pl.multiple_of(t * half_feat, half_feat), half_feat)
    far_cols = pl.ds(pl.multiple_of(other * half_feat, half_feat), half_feat)

    def norm_rows(i, _):
        at = pl.ds(pl.multiple_of(i * step_rows, step_rows), step_rows)
        own = tok_ref[at, :].astype(f32)
        far = tok_in[at, :].astype(f32)
        total = jnp.sum(own * own, axis=1, keepdims=True) + jnp.sum(far * far, axis=1, keepdims=True)
        scale = lax.rsqrt(total / (2 * half_feat) + epsilon)
        nrm[at, own_cols] = (own * scale * gain_ref[:, own_cols]).astype(bf16)
        nrm[at, far_cols] = (far * scale * gain_ref[:, far_cols]).astype(bf16)
        return 0

    lax.fori_loop(0, rows // step_rows, norm_rows, 0)

    my_rows = pl.ds(pl.multiple_of(t * half, half), half)
    cut = rows * 7 // 16
    core_rows = (pl.ds(0, cut), pl.ds(cut, rows - cut))

    def feature_block(index):
        return pl.ds(pl.multiple_of(index * block, block), block)

    def a2a_copy(core, r, which):
        lines = core_rows[core]
        to = flip(2 - r)
        return remote(
            nrm.at[lines, feature_block(to if which == 0 else flip(3))],
            xg.at[r, which, lines],
            send_s.at[0],
            a2a_r.at[which],
            {"fs": to},
        )

    def fwd_copy(core, r, which):
        lines = core_rows[core]
        return remote(
            xg.at[r, which, lines], xg.at[r, which, lines], send_s.at[0], fwd_r.at[0], {"tp": other}
        )

    def a2a_start(core):
        for r in range(2):
            for which in range(2):
                a2a_copy(core, r, which).start()

    on_core(0, lambda: a2a_start(0))
    on_core(1, lambda: a2a_start(1))
    loaded(wm.at[pl.ds(QUERY, 2)], 4)
    send_weights(third, parity, splits + 1)
    loaded(ws, 3)
    normed = nrm[...]
    queries[0] = dot(normed, ws[0]).astype(bf16)

    def query_copy():
        return remote(queries.at[0], queries.at[1], far_s.at[0], far_r.at[0], {"sp": s - 1})

    def kv_copy(d):
        return remote(kv.at[d - 1], kv.at[d], kv_s.at[d - 1], kv_r.at[d - 1], {"sp": s + 1})

    def kv_send(d):
        @pl.when((s < helper) & (s >= d - 1))
        def _():
            kv_copy(d).start()

    def kv_project():
        normed = nrm[...]
        kv[0, 0] = dot(normed, ws[1]).astype(bf16)
        kv[0, 1] = dot(normed, ws[2]).astype(bf16)
        kv_send(1)

    def pass_first():
        for c in range(splits):
            pass_weights(first, first_lines(c), c)

    on_core(0, kv_project)
    pass_first()
    on_core(1, kv_project)

    row_at = lax.broadcasted_iota(jnp.int32, (rows, rows), 0)
    col_at = lax.broadcasted_iota(jnp.int32, (rows, rows), 1)
    loaded(gate_in, 5)
    loaded(shift_ref, 8)
    load(bias_hbm, bias_ref, 6).wait()
    load(sbias_hbm, sbias_ref, 7).wait()
    gw[...] = jnp.zeros(gw.shape, bf16)
    gw[0:heads, :] = gate_in[0]
    gw[8 : 8 + heads, :] = gate_in[1]
    gate = dot(gw[...], normed, ((1,), (1,)))
    triu = (row_at <= col_at).astype(f32)
    u_rows[...] = jnp.zeros(u_rows.shape, f32)
    for h in range(heads):
        log_forget = shift_ref[h : h + 1, :] - softplus(-(gate[8 + h : 9 + h, :] + bias_ref[0:1, h : h + 1]))
        cumulative = lax.dot_general(
            jnp.broadcast_to(log_forget, (8, rows)), triu, (((1,), (0,)), ((), ())),
            precision=lax.Precision.HIGHEST, preferred_element_type=f32,
        )
        u_rows[h : h + 1, :] = gate[h : h + 1, :] - cumulative[0:1, :]
        totals[h : h + 1, :] = jnp.broadcast_to(
            cumulative[0:1, rows - 1 : rows], (1, totals.shape[1])
        )
    u_cols[...] = jnp.transpose(u_rows[...])

    pass_weights(second, parity, splits)

    @pl.when(s == last)
    def _():
        query_copy().start()


    def stick_part(at, h, kv_at, diagonal):
        cols = slice(h * ds, (h + 1) * ds)
        z = dot(queries[at, :, cols], kv[kv_at, 0, :, cols], ((1,), (1,)))
        z = z * ds ** (-0.5) + sbias_ref[0:1, h : h + 1]
        keep = -softplus(z)
        visible = col_at < row_at
        if diagonal:
            kept = jnp.where(visible, keep, 0.0)
        else:
            kept = keep
        strict = (row_at > col_at).astype(bf16)
        high = kept.astype(bf16)
        low = (kept - high.astype(f32)).astype(bf16)
        after = dot(high, strict) + dot(low, strict)
        weights = jnp.exp(z + keep + after)
        if diagonal:
            weights = jnp.where(visible, weights, 0.0)
        part = dot(weights.astype(bf16), kv[kv_at, 1, :, cols])
        return part, after[:, 0:1] + kept[:, 0:1]

    def stick_first(at, diagonal):
        for h in range(heads):
            part, keep = stick_part(at, h, 0, diagonal)
            stick_acc[at, h] = part
            stick_run[at, h] = jnp.broadcast_to(keep, stick_run.shape[2:])

    def kv_forward(d):
        @pl.when((s >= d) & (s <= helper))
        def _():
            remote(kv.at[d - 1], kv.at[d], kv_s.at[d - 1], kv_r.at[d - 1], {"sp": s - 1}).wait_recv()

        @pl.when((s >= d) & (s < helper))
        def _():
            kv_copy(d + 1).start()

    def stick_span(at, d):
        for h in range(heads):
            part, keep = stick_part(at, h, d, False)
            stick_acc[at, h] = stick_acc[at, h] + jnp.exp(stick_run[at, h]) * part
            stick_run[at, h] = stick_run[at, h] + keep

    def own_span(d):
        @pl.when((s >= d) & (s <= helper))
        def _():
            stick_span(0, d)

    def far_span(d):
        @pl.when(s == helper)
        def _():
            stick_span(1, d)

    def over(low, high, step):
        if high > low:
            lax.fori_loop(low, high, lambda d, c: (step(d), c)[1], 0)

    loaded(wout, 9)
    wout_copy = remote(wout, wout_in, send_s.at[3], tok_r.at[1], {"tp": other})
    wout_copy.start()
    stick_first(0, True)

    def a2a_forward(core):
        for which in range(2):
            await_bytes(xg.at[:, which, core_rows[core]], a2a_r.at[which])
            for r in range(2):
                fwd_copy(core, r, which).start()

    on_core(0, lambda: a2a_forward(0))
    on_core(1, lambda: a2a_forward(1))
    far_rows = pl.ds(pl.multiple_of(other * half, half), half)

    def rs_sem(p, h):
        return h if p < 2 else p + (h if p == GATE else 0)

    def rs_copy(p, h, lines):
        return remote(
            sb.at[p, h, lines], rb.at[p, h, lines], send_s.at[1], rs_r.at[rs_sem(p, h)],
            {"fs": flip(sum_bits(p, h))},
        )

    def partials(items):
        rest_weights(items)
        for p, h in items:
            cols = slice(h * dm, (h + 1) * dm)
            r = role(p, h)
            sb[p, h] = (dot(xg[r, 0], wm[p, :, cols]) + dot(xg[r, 1], wg[p, h])).astype(bf16)
            rs_copy(p, h, pl.ds(0, rows)).start()

    def first_partials(items, core):
        for at in (core, 1 - core):
            lines = core_rows[at]
            if at != core:
                await_bytes(xg.at[:, :, lines], fwd_r.at[0])
            for p, h in items:
                cols = slice(h * dm, (h + 1) * dm)
                r = role(p, h)
                sb[p, h, lines] = (
                    dot(xg[r, 0, lines], wm[p, :, cols]) + dot(xg[r, 1, lines], wg[p, h])
                ).astype(bf16)
                rs_copy(p, h, lines).start()

    def own_partials(items):
        for p, h in items:
            cols = slice(h * dm, (h + 1) * dm)
            own_part[p, h] = dot(nrm[:, feature_block(f)], wm[p, :, cols]) + dot(
                nrm[:, feature_block(flip(pair_bits(p, h)))], wg[p, h]
            )

    def finish(p, h):
        return (own_part[p, h] + rb[p, h].astype(f32)).astype(bf16)

    def column(h):
        return u_cols[:, h : h + 1]

    def own_state(h):
        await_bytes(rb.at[pl.ds(0, 2), h], rs_r.at[h])
        proj[KEY, h] = (finish(KEY, h).astype(f32) * dm ** (-0.5)).astype(bf16)
        proj[VALUE, h] = finish(VALUE, h)
        u = column(h)
        top = jnp.max(u, axis=0, keepdims=True)
        weighted = (proj[KEY, h].astype(f32) * jnp.exp(u - top)).astype(bf16)
        state_own[h] = dot(weighted, proj[VALUE, h], ((0,), (0,)))

    def log_copy(h, to):
        return remote(log_out.at[h], log_in.at[h], log_s.at[0], log_r.at[h], {"sp": to})

    piece_dm = dm // 2
    pieces = 4

    def chain_copy(h, c, to):
        lines = pl.ds(c // 2 * piece_dm, piece_dm)
        cols = pl.ds(c % 2 * piece_dm, piece_dm)
        at = h * pieces + c
        return remote(
            state_out.at[h, lines, cols], state_in.at[h, lines, cols], chain_s.at[0], chain_r.at[at],
            {"sp": to},
        )

    def chain_logs(h):
        @pl.when(s == 0)
        def _():
            log_in[h] = jnp.full(log_in.shape[1:], floor_neg, f32)
            state_in[h] = jnp.zeros(state_in.shape[1:], bf16)

        @pl.when(s > 0)
        def _():
            log_copy(h, s - 1).wait_recv()

        total = totals[h : h + 1, 0:1]
        early = total + log_in[h, 0:1, 0:1]
        late = total + jnp.max(column(h), axis=0, keepdims=True)
        top = jnp.maximum(early, late)

        @pl.when(s < last)
        def _():
            log_out[h] = jnp.broadcast_to(top, log_out.shape[1:])
            log_copy(h, s + 1).start()

        factors[h, 0] = jnp.broadcast_to(jnp.exp(early - top), factors.shape[2:])
        factors[h, 1] = jnp.broadcast_to(jnp.exp(late - top), factors.shape[2:])

    def chain(h, low=0, high=pieces):
        if low == 0:
            chain_logs(h)
        early, late = factors[h, 0, 0:1, 0:1], factors[h, 1, 0:1, 0:1]
        for c in range(low, high):
            lines = pl.ds(c // 2 * piece_dm, piece_dm)
            cols = pl.ds(c % 2 * piece_dm, piece_dm)

            @pl.when(s > 0)
            def _():
                chain_copy(h, c, s - 1).wait_recv()

            @pl.when(s < last)
            def _():
                state_out[h, lines, cols] = (
                    early * state_in[h, lines, cols].astype(f32) + late * state_own[h, lines, cols]
                ).astype(bf16)
                chain_copy(h, c, s + 1).start()

    def chain_if(where, h, low=0, high=pieces):
        @pl.when(where)
        def _():
            chain(h, low, high)

    over(1, min(2, n_sp - 1), kv_forward)
    rest_weights(first)
    on_core(0, lambda: first_partials(first, 0))
    on_core(1, lambda: first_partials(first, 1))
    send_weights(fourth, fourth_own, splits + 2)
    own_partials(first)
    pass_weights(third, parity, splits + 1)
    over(1, min(2, n_sp - 1), own_span)
    partials(second)
    def send_fourth():
        send_weights(fourth, fourth_all, splits + 3)

        @pl.when(s >= helper)
        def _():
            send_weights(fourth, fourth_rest, splits + 3)

    send_fourth()
    own_partials(second)
    @pl.when(s == helper)
    def _():
        query_copy().wait_recv()
        stick_first(1, False)

    over(1, min(2, n_sp - 1), far_span)

    @pl.when(s == helper)
    def _():
        pass_weights(fourth, fourth_own, splits + 2, 1)

    over(2, n_sp - 1, kv_forward)
    over(2, n_sp - 1, far_span)

    @pl.when(s == helper)
    def _():
        far_out[...] = stick_acc[1].astype(bf16)
        remote(far_out, far_in, far_s.at[0], far_r.at[0], {"sp": s + 1}).start()

    own_state(0)
    chain_if(s == 0, 0)

    @pl.when((s > 0) & (s < helper) & (t == 0))
    def _():
        pass_weights(fourth, fourth_own, splits + 2, 1)

    chain_if(s == 1, 0)
    own_state(1)
    chain_if(s == 0, 1)
    @pl.when((s > 0) & (s < helper) & (t == 1))
    def _():
        pass_weights(fourth, fourth_own, splits + 2, 1)

    partials(third)
    chain_if(s == 2, 0)
    own_partials(third)
    chain_if(s == 1, 1)

    @pl.when((s == 0) | (s == last))
    def _():
        await_bytes(both(GATE, 0, fourth_own), w_r.at[splits + 2])

    partials(fourth)
    own_partials(fourth)
    loaded(gains, 10)
    chain_if((s == 2) & (t == 1), 1)
    over(2, n_sp - 1, own_span)
    chain_if((s == 2) & (t == 0), 1, 0, 2)
    width = heads * dm

    def mix_copy(at, low, high):
        return remote(
            mix.at[far_rows, pl.ds(low, high - low)], mix_in.at[:, pl.ds(low, high - low)],
            send_s.at[2], out_r.at[at], {"tp": other},
        )

    def stick_mix():
        for h in range(heads):
            cols = slice(h * ds, (h + 1) * ds)
            out = stick_acc[0, h]
            scale = lax.rsqrt(jnp.mean(out * out, axis=1, keepdims=True) + epsilon)
            mix[:, heads * dm + h * ds : heads * dm + (h + 1) * ds] = (
                out * scale * gains[:, heads * dm + h * ds : heads * dm + (h + 1) * ds]
            ).astype(bf16)
        mix_copy(heads, width, width + heads * ds).start()
        early_out[...] = dot(mix[my_rows, width:], wout[width:, :])

    @pl.when(s < last)
    def _():
        stick_mix()

    chain_if((s == 2) & (t == 0), 1, 2, pieces)

    causal = col_at <= row_at
    await_bytes(rb.at[QUERY], rs_r.at[QUERY])
    for h in range(heads):
        proj[QUERY, h] = finish(QUERY, h)
        masked = jnp.where(causal, u_rows[h : h + 1, :], floor_neg)
        top = jnp.max(masked, axis=1, keepdims=True)
        scores = dot(proj[QUERY, h], proj[KEY, h], ((1,), (1,))) * jnp.exp(masked - top)
        own_part[QUERY, h] = dot(scores.astype(bf16), proj[VALUE, h])
        tops[h] = jnp.broadcast_to(top, tops.shape[1:])


    @pl.when(s == last)
    def _():
        remote(far_out, far_in, far_s.at[0], far_r.at[0], {"sp": s - 1}).wait_recv()
        for h in range(heads):
            stick_acc[0, h] = stick_acc[0, h] + jnp.exp(stick_run[0, h]) * far_in[h].astype(f32)
        stick_mix()

    wout_copy.wait_recv()

    def mix_head(h, lines):
        carried_max = log_in[h, 0:1, 0:1]
        top = tops[h, lines, 0:1]
        running = jnp.maximum(carried_max, top)
        total = jnp.exp(top - running) * own_part[QUERY, h, lines] + jnp.exp(
            carried_max - running
        ) * dot(proj[QUERY, h, lines], state_in[h])
        gate = (own_part[GATE, h, lines] + rb[GATE, h, lines].astype(f32)).astype(bf16)
        gated = total / (1.0 + jnp.exp(-gate.astype(f32)))
        scale = lax.rsqrt(jnp.mean(gated * gated, axis=1, keepdims=True) + epsilon)
        cols = slice(h * dm, (h + 1) * dm)
        mix[lines, cols] = (gated * scale * gains[:, cols]).astype(bf16)

    for h in range(heads):
        chain_if(s > 2, h)
        if h == 0:
            mix_copy(heads, width, width + heads * ds).wait_recv()
            early_out[...] = early_out[...] + dot(mix_in[:, width:], wout_in[width:, :])
        await_bytes(rb.at[GATE, h], rs_r.at[GATE + h])
        mix_head(h, far_rows)
        mix_copy(h, h * dm, (h + 1) * dm).start()
    for h in range(heads):
        mix_head(h, my_rows)

    early_out[...] = early_out[...] + dot(mix[my_rows, :width], wout[:width, :])
    for h in range(heads):
        cols = slice(h * dm, (h + 1) * dm)
        mix_copy(h, h * dm, (h + 1) * dm).wait_recv()
        total = early_out[...] + dot(mix_in[:, cols], wout_in[cols, :])
        if h < heads - 1:
            early_out[...] = total
        else:
            out_ref[...] = total.astype(bf16)

    def sent_rows(where, count, sem):
        @pl.when(where)
        def _():
            sent_bytes(wout.at[pl.ds(0, count)], sem)

    quarter = block * width // (4 * features)
    moved = [8 * lines * block // features for lines in (cut, rows - cut)]
    for core in range(2):
        sent_rows((t == core) & (s < helper), moved[core] + 9 * quarter, send_s.at[0])
        sent_rows((t == core) & (s >= helper), moved[core] + 10 * quarter, send_s.at[0])
    sums = 4 * rows * width // features
    sent_rows(s == 0, sums, send_s.at[1])
    sent_rows((s > 0) & (s < helper), sums + 7 * quarter, send_s.at[1])
    sent_rows(s == helper, sums + 13 * quarter, send_s.at[1])
    sent_rows(s == last, sums + 6 * quarter, send_s.at[1])
    sent_bytes(wout.at[pl.ds(0, (rows * half_feat + half * wout.shape[0]) // features)], send_s.at[2])
    wout_copy.wait_send()

    @pl.when(s == helper)
    def _():
        remote(far_out, far_in, far_s.at[0], far_r.at[0], {"sp": s + 1}).wait_send()

    @pl.when(s == last)
    def _():
        query_copy().wait_send()

    @pl.when(s < last)
    def _():
        sent_bytes(log_out, log_s.at[0])
        sent_bytes(state_out, chain_s.at[0])

    def kv_done(d, c):
        @pl.when((s < helper) & (s >= d - 1))
        def _():
            kv_copy(d).wait_send()

        return c

    lax.fori_loop(1, n_sp - 1, kv_done, 0)


def per_device(
    n_sp,
    tokens,
    norm_gain,
    memory_query,
    memory_key,
    memory_value,
    memory_outgate,
    memory_ingate,
    memory_forget,
    forget_bias,
    forget_shift,
    stick_query,
    stick_key,
    stick_value,
    stick_bias,
    memory_gain,
    stick_gain,
    out_memory,
    out_stick,
):
    rows, half_feat = tokens.shape[1:]
    features = 2 * half_feat
    heads = forget_bias.shape[0]
    block, width = memory_query.shape
    dm = width // heads
    stick_width = stick_query.shape[1]
    ds = stick_width // heads
    lanes = 128
    half = rows // 2

    vmem = pl.BlockSpec(memory_space=pltpu.VMEM)
    anyw = pl.BlockSpec(memory_space=pl.ANY)
    dma = pltpu.SemaphoreType.DMA
    out = pl.pallas_call(
        functools.partial(kernel, n_sp),
        out_shape=pltpu.VMEM((half, features), bf16),
        in_specs=[anyw] * 18,
        out_specs=vmem,
        scratch_shapes=[
            pltpu.VMEM((rows, half_feat), bf16),
            pltpu.VMEM((1, features), f32),
            pltpu.VMEM((2, heads, features), bf16),
            pltpu.VMEM((heads, rows), f32),
            pltpu.VMEM((1, heads), f32),
            pltpu.VMEM((1, heads), f32),
            pltpu.VMEM((1, width + stick_width), f32),
            pltpu.VMEM((rows, half_feat), bf16),
            pltpu.VMEM((rows, features), bf16),
            pltpu.VMEM((2, 2, rows, block), bf16),
            pltpu.VMEM((4, block, width), bf16),
            pltpu.VMEM((4, heads, block, dm), bf16),
            pltpu.VMEM((3, features, stick_width), bf16),
            pltpu.VMEM((width + stick_width, features), bf16),
            pltpu.VMEM((4, heads, rows, dm), bf16),
            pltpu.VMEM((4, heads, rows, dm), bf16),
            pltpu.VMEM((4, heads, rows, dm), f32),
            pltpu.VMEM((4, heads, rows, dm), bf16),
            pltpu.VMEM((2, rows, stick_width), bf16),
            pltpu.VMEM((n_sp - 1, 2, rows, stick_width), bf16),
            pltpu.VMEM((2, heads, rows, ds), f32),
            pltpu.VMEM((2, heads, rows, ds), f32),
            pltpu.VMEM((heads, rows, ds), bf16),
            pltpu.VMEM((heads, rows, ds), bf16),
            pltpu.VMEM((16, features), bf16),
            pltpu.VMEM((lanes, rows), f32),
            pltpu.VMEM((rows, lanes), f32),
            pltpu.VMEM((8, lanes), f32),
            pltpu.VMEM((heads, rows, lanes), f32),
            pltpu.VMEM((heads, dm, dm), f32),
            pltpu.VMEM((heads, dm, dm), bf16),
            pltpu.VMEM((heads, dm, dm), bf16),
            pltpu.VMEM((heads, 8, lanes), f32),
            pltpu.VMEM((heads, 8, lanes), f32),
            pltpu.VMEM((heads, 2, 8, lanes), f32),
            pltpu.VMEM((rows, width + stick_width), bf16),
            pltpu.VMEM((half, width + stick_width), bf16),
            pltpu.VMEM((width + stick_width, features), bf16),
            pltpu.VMEM((half, features), f32),
            dma((11,)),
            dma((4,)),
            dma((2,)),
            dma((2,)),
            dma((1,)),
            dma((6,)),
            dma((4,)),
            dma((5,)),
            dma((n_sp - 2,)),
            dma((n_sp - 2,)),
            dma((1,)),
            dma((1,)),
            dma((1,)),
            dma((4 * heads,)),
            dma((1,)),
            dma((heads,)),
            dma((heads + 1,)),
        ],
        compiler_params=pltpu.CompilerParams(
            collective_id=0, has_side_effects=True, vmem_limit_bytes=60 * 1024 * 1024
        ),
    )(
        tokens[0],
        norm_gain[None],
        memory_ingate.T,
        memory_forget.T,
        forget_bias[None],
        forget_shift[0].T,
        stick_bias[None],
        memory_gain[None],
        stick_gain[None],
        memory_key,
        memory_value,
        memory_query,
        memory_outgate,
        stick_query,
        stick_key,
        stick_value,
        out_memory,
        out_stick,
    )
    return out[None]


def solution(mesh):
    assert mesh.shape["fs"] == 4 and mesh.shape["tp"] == 2
    return jax.shard_map(
        functools.partial(per_device, mesh.shape["sp"]),
        mesh=mesh,
        in_specs=(
            P("fs", "sp", "tp"),
            P(),
            P("fs", "tp"),
            P("fs", "tp"),
            P("fs", "tp"),
            P("fs", "tp"),
            P(None, "tp"),
            P(None, "tp"),
            P("tp"),
            P("fs", "sp", "tp"),
            P(None, "tp"),
            P(None, "tp"),
            P(None, "tp"),
            P("tp"),
            P("tp"),
            P("tp"),
            P("tp", None),
            P("tp", None),
        ),
        out_specs=P("fs", ("sp", "tp"), None),
        check_vma=False,
    )
```
